256 devices in a mesh: sp: 32 (over z, y), tp: 8 (over x, core).
Axes of the slice: x: 4, y: 4, z: 8, core: 2. Of those that a mesh axis runs over, the one named last changes fastest.
Arguments:
- tokens: bfloat16 [32768, 2048], P('sp'), may hold values from -6 to 6
- in_gain: float32 [2048], replicated, may hold values from 0.1 to 1.9
- w_query: bfloat16 [2048, 1024], P(None, 'tp'), may hold values from -0.125 to 0.125
- w_forget: bfloat16 [2048, 1024], P(None, 'tp'), may hold values from -0.125 to 0.125
- w_input: bfloat16 [2048, 1024], P(None, 'tp'), may hold values from -0.125 to 0.125
- w_outgate: bfloat16 [2048, 1024], P(None, 'tp'), may hold values from -0.125 to 0.125
- w_conv_h: bfloat16 [2048, 1024], P(None, 'tp'), may hold values from -0.125 to 0.125
- w_conv_b: bfloat16 [2048, 1024], P(None, 'tp'), may hold values from -0.125 to 0.125
- w_conv_c: bfloat16 [2048, 1024], P(None, 'tp'), may hold values from -0.125 to 0.125
- forget_floor: float32 [1024], P('tp'), may hold values from 0.84 to 1
- forget_leak: float32 [32768, 1024], P('sp', 'tp'), may hold values from -1 to 0
- state_gain: float32 [128], replicated, may hold values from 0.1 to 1.9
- conv_taps: bfloat16 [3, 1024], P(None, 'tp'), may hold values from -3.5 to 3.5
- group_gain: float32 [128], replicated, may hold values from 0.1 to 1.9
- out_state: bfloat16 [1024, 2048], P('tp'), may hold values from -0.1875 to 0.1875
- out_conv: bfloat16 [1024, 2048], P('tp'), may hold values from -0.1875 to 0.1875
Outputs:
- mixed_out: bfloat16 [32768, 2048], P('sp', 'tp')
The draws below stay inside these ranges and needn't reach their ends.
All inputs are finite; a program needn't handle non-finite values.
Results may differ from the reference program's by a relative error of at most 0.015.
Values may be sent and summed in bfloat16 or wider, within the bound.
No kernel may reach another device: no remote copies, remote signals or barrier semaphores. Data moves between devices by JAX's collectives and lax.ppermute only.
A program may use at most 128 MiB of HBM per device.

```python
import jax
import jax.numpy as jnp
from jax import lax

D = 2048
GROUP_FEATURES = 128
MIXER_COUNT = 8
CONV_CH = 1024
BLOCK = 64
TAPS = 3
TOK_DEV = 1024
STEP_COUNT = 32768
STATE_W = 1024
MIX = 2048


def draw_forget_floor(key, part):
    key_fast, key_gap, key_slow = jax.random.split(jax.random.fold_in(key, 11), 3)
    share = 0.5
    is_fast = jax.random.uniform(key_fast, (MIXER_COUNT,)) < share
    is_fast = jnp.repeat(is_fast, GROUP_FEATURES)
    fast_gap = jnp.exp(jax.random.uniform(key_gap, (STATE_W,), jnp.float32, jnp.log(0.05), jnp.log(0.15)))
    slow_gap = jnp.exp(jax.random.uniform(key_slow, (STATE_W,), jnp.float32, jnp.log(0.2), jnp.log(1.0))) / STEP_COUNT
    return (1.0 - jnp.where(is_fast, fast_gap, slow_gap)).astype(jnp.float32)


def draw_forget_leak(key, part):
    key_scale, random_seed_site, key_depth, key_jitter = jax.random.split(jax.random.fold_in(key, 23), 4)
    nblk = STEP_COUNT // TOK_DEV
    low, high = (jnp.log(0.5), jnp.log(2.0))
    block_scale = jnp.exp(jax.random.uniform(key_scale, (nblk, MIXER_COUNT), jnp.float32, low, high))
    block_scale = jnp.repeat(jnp.repeat(block_scale, TOK_DEV, axis=0), GROUP_FEATURES, axis=1)
    jitter = jax.random.uniform(key_jitter, (STEP_COUNT, STATE_W), jnp.float32, 0.5, 1.5)
    starting_shift = -0.2 / STEP_COUNT * block_scale * jitter
    span_start = jax.random.randint(random_seed_site, (3, MIXER_COUNT), 0, STEP_COUNT)
    layer_number = jax.random.uniform(key_depth, (3, MIXER_COUNT), jnp.float32, jnp.log(0.5), jnp.log(0.8))
    element_places = jnp.arange(STEP_COUNT)[:, None]
    span_sizes = jnp.zeros((STEP_COUNT, MIXER_COUNT), jnp.float32)
    for entry_number in range(3):
        span_sizes = span_sizes + jnp.where(element_places == span_start[entry_number][None, :], layer_number[entry_number][None, :], 0.0)
    return (starting_shift + jnp.repeat(span_sizes, GROUP_FEATURES, axis=1)).astype(jnp.float32)


def with_spikes(values, key, source, target, parts, factor):
    owner, partner = [(jnp.arange(values.shape[position]) // (values.shape[position] // parts)).reshape([-1 if axis == position else 1 for axis in range(values.ndim)]) for position in (source, target)]
    chosen = jax.random.permutation(key, parts)[partner]
    strong = (owner == chosen) | (owner == (partner + parts // 2) % parts)
    return jnp.where(strong, factor * values, values)


def levels(key, dims, pieces, least, largest):
    level, own = 1.0, jax.random.fold_in(key, 6)
    for dim, parts in pieces:
        steps = jnp.exp(jax.random.uniform(jax.random.fold_in(own, dim), (parts,), jnp.float32, least / len(pieces), largest / len(pieces)))
        level = level * jnp.repeat(steps, dims[dim] // parts).reshape([-1 if axis == dim else 1 for axis in range(len(dims))])
    return level


def centred(rng, extent, spread, reach, cuts=(), held_as=jnp.bfloat16):
    loudness = levels(rng, extent, cuts, -0.22, 0.18) if cuts else 1.0
    array = jax.random.normal(rng, extent, jnp.float32) * spread * loudness
    return jnp.minimum(jnp.maximum(array, -reach), reach).astype(held_as)


def heavy_noise(own_key, dims, width, limit, shards, heavy, dtype=jnp.bfloat16):
    values = width * jax.random.normal(own_key, dims, jnp.float32)
    if shards:
        values = values * levels(own_key, dims, shards, -0.22, 0.18)
    return jnp.clip(with_spikes(values, jax.random.fold_in(own_key, 3), *heavy), -limit, limit).astype(dtype)


def setup_inputs(seed: int = 0) -> dict:
    streams_of = jax.random.split(jax.random.key(seed), 17)
    return {
        "tokens": centred(streams_of[0], (STEP_COUNT, D), 1.0, 6.0, ((0, 32),)),
        "in_gain": jnp.clip(1.0 + 0.18 * jax.random.normal(streams_of[1], (D,), jnp.float32), 0.1, 1.9),
        "w_query": centred(streams_of[2], (D, STATE_W), D ** -0.5, 0.125, ((1, 8),)),
        "w_forget": centred(streams_of[3], (D, STATE_W), D ** -0.5, 0.125, ((1, 8),)),
        "w_input": centred(streams_of[4], (D, STATE_W), D ** -0.5, 0.125, ((1, 8),)),
        "w_outgate": centred(streams_of[5], (D, STATE_W), D ** -0.5, 0.125, ((1, 8),)),
        "w_conv_h": centred(streams_of[6], (D, CONV_CH), D ** -0.5, 0.125, ((1, 8),)),
        "w_conv_b": centred(streams_of[7], (D, CONV_CH), D ** -0.5, 0.125, ((1, 8),)),
        "w_conv_c": centred(streams_of[8], (D, CONV_CH), D ** -0.5, 0.125, ((1, 8),)),
        "forget_floor": draw_forget_floor(jax.random.fold_in(streams_of[16], 71), 0),
        "forget_leak": draw_forget_leak(jax.random.fold_in(streams_of[16], 71), 0),
        "state_gain": jnp.clip(1.0 + 0.18 * jax.random.normal(streams_of[11], (GROUP_FEATURES,), jnp.float32), 0.1, 1.9),
        "conv_taps": centred(streams_of[12], (TAPS, CONV_CH), TAPS ** -0.5, 3.5, ((1, 8),)),
        "group_gain": jnp.clip(1.0 + 0.18 * jax.random.normal(streams_of[13], (GROUP_FEATURES,), jnp.float32), 0.1, 1.9),
        "out_state": heavy_noise(streams_of[14], (STATE_W, D), MIX ** -0.5, 0.1875, ((0, 8),), (0, 1, 8, 2.0)),
        "out_conv": heavy_noise(streams_of[15], (CONV_CH, D), MIX ** -0.5, 0.1875, ((0, 8),), (0, 1, 8, 2.0)),
    }


norm_eps = 1e-06
highest = lax.Precision.HIGHEST

def rms_rows(values, gain):
    scale = lax.rsqrt(lax.optimization_barrier(jnp.mean(values * values, axis=-1, keepdims=True)) + norm_eps)
    return values * scale * gain.astype(jnp.float32)

def state_block(carry_state, inputs):
    query_blk, key_blk, value_blk, logf_blk = inputs
    cum_log = jnp.cumsum(logf_blk, axis=1)
    carried = jnp.einsum('hcd,hde->hce', query_blk * jnp.exp(cum_log), carry_state, precision=highest)
    length = logf_blk.shape[1]
    causal = (jnp.arange(length)[:, None] >= jnp.arange(length)[None, :])[None, :, :, None]
    diff_log = cum_log[:, :, None, :] - cum_log[:, None, :, :]
    decay_all = jnp.exp(jnp.where(causal, diff_log, -jnp.inf))
    scores = jnp.einsum('hid,hjd,hijd->hij', query_blk, key_blk, decay_all, precision=highest)
    result = carried + jnp.einsum('hij,hje->hie', scores, value_blk, precision=highest)
    last_log = cum_log[:, -1, :]
    fresh = jnp.einsum('hcd,hce->hde', key_blk * jnp.exp(last_log[:, None, :] - cum_log), value_blk, precision=highest)
    new_state = jnp.exp(last_log)[:, :, None] * carry_state + fresh
    return (new_state, result)

def reference(tokens, in_gain, w_query, w_forget, w_input, w_outgate, w_conv_h, w_conv_b, w_conv_c, forget_floor, forget_leak, state_gain, conv_taps, group_gain, out_state, out_conv):
    count = tokens.shape[0]
    heads = MIXER_COUNT
    normed = rms_rows(tokens.astype(jnp.float32), in_gain).astype(jnp.bfloat16)

    def project(weight):
        return jnp.dot(normed, weight, preferred_element_type=jnp.float32).astype(jnp.bfloat16)
    proj_query = project(w_query)
    proj_forget = project(w_forget)
    proj_input = project(w_input)
    proj_outgate = project(w_outgate)
    proj_h = project(w_conv_h)
    proj_b = project(w_conv_b)
    proj_c = project(w_conv_c)
    gate_logit = proj_forget.astype(jnp.float32)
    log_forget = jnp.logaddexp(jnp.log(forget_floor), jnp.log1p(-forget_floor) + jax.nn.log_sigmoid(gate_logit)) + forget_leak
    key_gate = (1.0 - forget_floor) * jax.nn.sigmoid(-gate_logit)
    query_act = jax.nn.silu(proj_query.astype(jnp.float32))
    value_f = proj_input.astype(jnp.float32)
    nblk = count // BLOCK

    def to_blocks(arr):
        return arr.reshape(nblk, BLOCK, heads, GROUP_FEATURES).transpose(0, 2, 1, 3)
    start_state = jnp.zeros((heads, GROUP_FEATURES, GROUP_FEATURES), jnp.float32)
    _, outputs = lax.scan(state_block, start_state, (to_blocks(query_act), to_blocks(key_gate), to_blocks(value_f), to_blocks(log_forget)))
    state_read = outputs.transpose(0, 2, 1, 3).reshape(count, heads, GROUP_FEATURES)
    out_gate = jax.nn.silu(proj_outgate.astype(jnp.float32)).reshape(count, heads, GROUP_FEATURES)
    state_res = (rms_rows(state_read, state_gain) * out_gate).reshape(count, STATE_W).astype(jnp.bfloat16)
    conv_in = (proj_c.astype(jnp.float32) * proj_h.astype(jnp.float32)).astype(jnp.bfloat16)
    padded = jnp.concatenate([jnp.zeros((TAPS - 1, CONV_CH), jnp.bfloat16), conv_in], axis=0).astype(jnp.float32)
    taps_f = conv_taps.astype(jnp.float32)
    conv_sum = jnp.zeros((count, CONV_CH), jnp.float32)
    for offset in range(TAPS):
        conv_sum = conv_sum + taps_f[offset][None, :] * padded[offset:offset + count]
    gated = (proj_b.astype(jnp.float32) * conv_sum).reshape(count, CONV_CH // GROUP_FEATURES, GROUP_FEATURES)
    conv_res = rms_rows(gated, group_gain).reshape(count, CONV_CH).astype(jnp.bfloat16)
    total = jnp.dot(state_res, out_state, preferred_element_type=jnp.float32)
    total = total + jnp.dot(conv_res, out_conv, preferred_element_type=jnp.float32)
    return total.astype(jnp.bfloat16)
```

```python
import jax
import jax.numpy as jnp
from jax import lax
from jax.experimental import pallas as pl
from jax.experimental.pallas import tpu as pltpu
from jax.sharding import Mesh
from jax.sharding import PartitionSpec as P


F = 128
BLOCK = 64
TAPS = 3
STEP = 256
PACK = F + 16
EPS = 1e-06
f32 = jnp.float32
bf16 = jnp.bfloat16


def dot(a, b, dims=((1,), (0,))):
    return lax.dot_general(a, b, (dims, ((), ())), preferred_element_type=f32)


def rms(values, gain):
    return values * lax.rsqrt(jnp.mean(values * values, axis=-1, keepdims=True) + EPS) * gain


def silu(x):
    return x * jax.nn.sigmoid(x)


def put_message(ref, state, decay):
    high = decay.astype(bf16)
    low = (decay - high.astype(f32)).astype(bf16)
    ref[:F] = state.astype(bf16)
    row = lax.broadcasted_iota(jnp.int32, (16, F), 0)
    ref[F:] = jnp.where(row == 0, high.astype(f32), jnp.where(row == 1, low.astype(f32), 0.0)).astype(bf16)


def get_message(ref):
    tail = ref[F:].astype(f32)
    return ref[:F].astype(f32), tail[0:1] + tail[1:2]


def front_kernel(tokens, gain, w_forget, w_input, floor, leak,
                 normed, keys, values, cums, starts, befores, message,
                 weights, state, total):
    step = pl.program_id(0)

    @pl.when(step == 0)
    def _():
        weights[:, :F] = w_forget[...]
        weights[:, F:] = w_input[...]
        state[...] = jnp.zeros_like(state)
        total[...] = jnp.zeros_like(total)

    n = rms(tokens[...].astype(f32), gain[...]).astype(bf16)
    normed[...] = n
    both = dot(n, weights[...]).astype(bf16)
    gate = both[:, :F].astype(f32)
    value = both[:, F:]
    values[...] = value
    key = (1.0 - floor[...]) * jax.nn.sigmoid(-gate)
    log_forget = jnp.log1p(-key) + leak[...]
    row = lax.broadcasted_iota(jnp.int32, (STEP, STEP), 0)
    col = lax.broadcasted_iota(jnp.int32, (STEP, STEP), 1)
    tri = jnp.where((row >= col) & ((row >> 6) == (col >> 6)), 1.0, 0.0).astype(bf16)
    high = log_forget.astype(bf16)
    rest = log_forget - high.astype(f32)
    mid = rest.astype(bf16)
    low = (rest - mid.astype(f32)).astype(bf16)
    cum = dot(tri, high) + dot(tri, mid) + dot(tri, low)
    cums[...] = cum
    for b in range(STEP // BLOCK):
        at = b * BLOCK
        c = cum[at : at + BLOCK]
        k = key[at : at + BLOCK]
        half = c[BLOCK // 2 - 1 : BLOCK // 2]
        last = c[BLOCK - 1 : BLOCK]
        keys[at : at + BLOCK] = (k * jnp.exp(half - c)).astype(bf16)
        fresh = dot(value[at : at + BLOCK], (k * jnp.exp(last - c)).astype(bf16), ((0,), (0,)))
        starts[b] = state[...].astype(bf16)
        befores[b] = total[...]
        state[...] = state[...] * jnp.exp(last) + fresh
        total[...] = total[...] + last

    @pl.when(step == pl.num_programs(0) - 1)
    def _():
        put_message(message, state[...], jnp.exp(total[0:1]))


def front(tokens, gain, w_forget, w_input, floor, leak):
    count, width = tokens.shape
    steps = count // STEP
    blocks = STEP // BLOCK
    whole = lambda s: (0, 0)
    line = lambda s: (s, 0)
    deep = lambda s: (s, 0, 0)
    return pl.pallas_call(
        front_kernel,
        grid=(steps,),
        in_specs=[
            pl.BlockSpec((STEP, width), line),
            pl.BlockSpec((1, width), whole),
            pl.BlockSpec((width, F), whole),
            pl.BlockSpec((width, F), whole),
            pl.BlockSpec((1, F), whole),
            pl.BlockSpec((STEP, F), line),
        ],
        out_specs=[
            pl.BlockSpec((STEP, width), line),
            pl.BlockSpec((STEP, F), line),
            pl.BlockSpec((STEP, F), line),
            pl.BlockSpec((STEP, F), line),
            pl.BlockSpec((blocks, F, F), deep),
            pl.BlockSpec((blocks, 8, F), deep),
            pl.BlockSpec((PACK, F), whole),
        ],
        out_shape=[
            jax.ShapeDtypeStruct((count, width), bf16),
            jax.ShapeDtypeStruct((count, F), bf16),
            jax.ShapeDtypeStruct((count, F), bf16),
            jax.ShapeDtypeStruct((count, F), f32),
            jax.ShapeDtypeStruct((count // BLOCK, F, F), bf16),
            jax.ShapeDtypeStruct((count // BLOCK, 8, F), f32),
            jax.ShapeDtypeStruct((PACK, F), bf16),
        ],
        scratch_shapes=[
            pltpu.VMEM((width, 2 * F), bf16),
            pltpu.VMEM((F, F), f32),
            pltpu.VMEM((8, F), f32),
        ],
        compiler_params=pltpu.CompilerParams(dimension_semantics=("arbitrary",)),
        name="front",
    )(tokens, gain, w_forget, w_input, floor, leak)


def read_kernel(normed, w_query, w_outgate, gain, keys, values, cums, starts, befores,
                reads, carries, gates, weights):
    @pl.when(pl.program_id(0) == 0)
    def _():
        weights[:, :F] = w_query[...]
        weights[:, F:] = w_outgate[...]

    both = dot(normed[...], weights[...]).astype(bf16).astype(f32)
    query = silu(both[:, :F])
    gates[...] = silu(both[:, F:]) * gain[...]
    row = lax.broadcasted_iota(jnp.int32, (BLOCK, BLOCK), 0)
    col = lax.broadcasted_iota(jnp.int32, (BLOCK, BLOCK), 1)
    for b in range(STEP // BLOCK):
        at = b * BLOCK
        q = query[at : at + BLOCK]
        c = cums[at : at + BLOCK]
        half = c[BLOCK // 2 - 1 : BLOCK // 2]
        scores = dot((q * jnp.exp(c - half)).astype(bf16), keys[at : at + BLOCK], ((1,), (1,)))
        scores = jnp.where(row >= col, scores, 0.0).astype(bf16)
        faded = q * jnp.exp(c)
        reads[at : at + BLOCK] = dot(scores, values[at : at + BLOCK]) + dot(
            faded.astype(bf16), starts[b], ((1,), (1,))
        )
        carries[at : at + BLOCK] = (faded * jnp.exp(befores[b, 0:1])).astype(bf16)


def read(normed, w_query, w_outgate, gain, keys, values, cums, starts, befores):
    count, width = normed.shape
    blocks = STEP // BLOCK
    whole = lambda s: (0, 0)
    line = lambda s: (s, 0)
    deep = lambda s: (s, 0, 0)
    return pl.pallas_call(
        read_kernel,
        grid=(count // STEP,),
        in_specs=[
            pl.BlockSpec((STEP, width), line),
            pl.BlockSpec((width, F), whole),
            pl.BlockSpec((width, F), whole),
            pl.BlockSpec((1, F), whole),
            pl.BlockSpec((STEP, F), line),
            pl.BlockSpec((STEP, F), line),
            pl.BlockSpec((STEP, F), line),
            pl.BlockSpec((blocks, F, F), deep),
            pl.BlockSpec((blocks, 8, F), deep),
        ],
        out_specs=[pl.BlockSpec((STEP, F), line)] * 3,
        out_shape=[
            jax.ShapeDtypeStruct((count, F), f32),
            jax.ShapeDtypeStruct((count, F), bf16),
            jax.ShapeDtypeStruct((count, F), f32),
        ],
        scratch_shapes=[pltpu.VMEM((width, 2 * F), bf16)],
        compiler_params=pltpu.CompilerParams(dimension_semantics=("arbitrary",)),
        name="read",
    )(normed, w_query, w_outgate, gain, keys, values, cums, starts, befores)


def conv_kernel(first, normed, rim, in_gain, w_h, w_c, w_b, taps, gain, result, weights, window):
    step = pl.program_id(0)

    @pl.when(step == 0)
    def _():
        weights[:, :F] = w_h[...]
        weights[:, F:] = w_c[...]
        edge = rms(rim[...].astype(f32), in_gain[...]).astype(bf16)
        both = dot(edge, weights[...]).astype(bf16).astype(f32)
        signal = (both[:, :F] * both[:, F:]).astype(bf16).astype(f32)
        window[:8] = jnp.where(first[0] > 0, 0.0, signal[8:])

    @pl.when(step > 0)
    def _():
        window[:8] = window[STEP:]

    both = dot(normed[...], weights[...]).astype(bf16).astype(f32)
    window[8:] = (both[:, :F] * both[:, F:]).astype(bf16).astype(f32)
    scale = taps[...].astype(f32)
    total = scale[0:1] * window[6 : 6 + STEP]
    total = total + scale[1:2] * window[7 : 7 + STEP]
    total = total + scale[2:3] * window[8 : 8 + STEP]
    after = dot(normed[...], w_b[...]).astype(bf16).astype(f32)
    result[...] = rms(after * total, gain[...]).astype(bf16)


def conv(first, normed, rim, in_gain, w_h, w_c, w_b, taps, gain):
    count, width = normed.shape
    whole = lambda s: (0, 0)
    line = lambda s: (s, 0)
    return pl.pallas_call(
        conv_kernel,
        grid=(count // STEP,),
        in_specs=[
            pl.BlockSpec(memory_space=pltpu.SMEM),
            pl.BlockSpec((STEP, width), line),
            pl.BlockSpec((16, width), whole),
            pl.BlockSpec((1, width), whole),
            pl.BlockSpec((width, F), whole),
            pl.BlockSpec((width, F), whole),
            pl.BlockSpec((width, F), whole),
            pl.BlockSpec((TAPS, F), whole),
            pl.BlockSpec((1, F), whole),
        ],
        out_specs=pl.BlockSpec((STEP, F), line),
        out_shape=jax.ShapeDtypeStruct((count, F), bf16),
        scratch_shapes=[pltpu.VMEM((width, 2 * F), bf16), pltpu.VMEM((STEP + 8, F), f32)],
        compiler_params=pltpu.CompilerParams(dimension_semantics=("arbitrary",)),
        name="conv",
    )(first, normed, rim, in_gain, w_h, w_c, w_b, taps, gain)


def row_kernel(index, own, one, two, three, total, before, fade):
    y = index[0]
    parts = [get_message(r) for r in (own, one, two, three)]
    place = [jnp.where(y >= d, y - d, y - d + 4) for d in range(4)]
    whole, inside = 0.0, 0.0
    product, product_before = 1.0, 1.0
    for d, (state, decay) in enumerate(parts):
        later = jnp.ones_like(decay)
        between = jnp.ones_like(decay)
        for other, (_, factor) in enumerate(parts):
            if other == d:
                continue
            behind = place[other] > place[d]
            later = later * jnp.where(behind, factor, 1.0)
            between = between * jnp.where(behind & (place[other] < y), factor, 1.0)
        whole = whole + state * later
        inside = inside + state * jnp.where(place[d] < y, between, 0.0)
        product = product * decay
        product_before = product_before * jnp.where(place[d] < y, decay, 1.0)
    put_message(total, whole, product)
    before[...] = inside
    fade[...] = jnp.broadcast_to(product_before, fade.shape)


def column_kernel(index, own, one, two, three, window, before, fade):
    z = index[0]
    state, product = jnp.zeros((F, F), f32), jnp.ones((1, F), f32)
    for d, ref in ((3, three), (2, two), (1, one)):
        piece, decay = get_message(ref)
        decay = jnp.where(z >= d, decay, 1.0)
        state = state * decay + jnp.where(z >= d, piece, 0.0)
        product = product * decay
    piece, decay = get_message(own)
    put_message(window, state * decay + piece, product * decay)
    before[...] = state
    fade[...] = jnp.broadcast_to(product, fade.shape)


def join(kernel, name, index, *messages):
    vmem = pl.BlockSpec(memory_space=pltpu.VMEM)
    return pl.pallas_call(
        kernel,
        in_specs=[pl.BlockSpec(memory_space=pltpu.SMEM)] + [vmem] * 4,
        out_specs=[vmem] * 3,
        out_shape=[
            jax.ShapeDtypeStruct((PACK, F), bf16),
            jax.ShapeDtypeStruct((F, F), f32),
            jax.ShapeDtypeStruct((8, F), f32),
        ],
        name=name,
    )(index, *messages)


def finish_kernel(index, far, column, column_fade, row, row_fade, carries, reads, gates, result):
    piece, _ = get_message(far)
    piece = jnp.where(index[0] >= 4, piece, 0.0)
    incoming = (column[...] + piece * column_fade[0:1]) * row_fade[0:1] + row[...]
    found = reads[...] + dot(carries[...], incoming.astype(bf16), ((1,), (1,)))
    result[...] = rms(found, gates[...]).astype(bf16)


def finish(index, far, column, column_fade, row, row_fade, carries, reads, gates):
    vmem = pl.BlockSpec(memory_space=pltpu.VMEM)
    return pl.pallas_call(
        finish_kernel,
        in_specs=[pl.BlockSpec(memory_space=pltpu.SMEM)] + [vmem] * 8,
        out_specs=vmem,
        out_shape=jax.ShapeDtypeStruct(reads.shape, bf16),
        name="finish",
    )(index, far, column, column_fade, row, row_fade, carries, reads, gates)


def half_kernel(*refs):
    parts, weights, out = refs[:4], refs[4:8], refs[8]
    out[...] = dot(
        jnp.concatenate([r[...] for r in parts], axis=1),
        jnp.concatenate([r[...] for r in weights], axis=0),
    )


def last_kernel(*refs):
    parts, weights, earlier, kept, sent = refs[:4], refs[4:8], refs[8], refs[9], refs[10]
    total = earlier[...] + dot(
        jnp.concatenate([r[...] for r in parts], axis=1),
        jnp.concatenate([r[...] for r in weights], axis=0),
    )
    width = total.shape[1] // 2
    kept[...] = total[:, :width]
    sent[...] = total[:, width:].astype(bf16)


def project_half(parts, weights):
    vmem = pl.BlockSpec(memory_space=pltpu.VMEM)
    return pl.pallas_call(
        half_kernel,
        in_specs=[vmem] * 8,
        out_specs=vmem,
        out_shape=jax.ShapeDtypeStruct((parts[0].shape[0], weights[0].shape[1]), f32),
        name="half",
    )(*parts, *weights)


def project_last(parts, weights, earlier):
    vmem = pl.BlockSpec(memory_space=pltpu.VMEM)
    count, width = earlier.shape
    return pl.pallas_call(
        last_kernel,
        in_specs=[vmem] * 9,
        out_specs=[vmem] * 2,
        out_shape=[
            jax.ShapeDtypeStruct((count, width // 2), f32),
            jax.ShapeDtypeStruct((count, width // 2), bf16),
        ],
        name="last",
    )(*parts, *weights, earlier)


def turned(array, axis, by):
    count = lax.axis_size(axis)
    return lax.ppermute(array, axis, [(i, (i + by) % count) for i in range(count)])


def body(
    tokens,
    in_gain,
    w_query,
    w_forget,
    w_input,
    w_outgate,
    w_conv_h,
    w_conv_b,
    w_conv_c,
    forget_floor,
    forget_leak,
    state_gain,
    conv_taps,
    group_gain,
    out_state,
    out_conv,
):
    x, c = lax.axis_index("x"), lax.axis_index("c")
    y, z = lax.axis_index("y"), lax.axis_index("z")
    here_y = y.astype(jnp.int32).reshape(1)
    here_z = z.astype(jnp.int32).reshape(1)
    first = ((y == 0) & (z == 0)).astype(jnp.int32).reshape(1)
    chips = lax.axis_size("x")
    width = tokens.shape[1] // chips
    gain_row = in_gain.reshape(1, -1)

    normed, keys, values, cums, starts, befores, message = front(
        tokens, gain_row, w_forget, w_input, forget_floor.reshape(1, -1), forget_leak
    )
    rim = turned(tokens[-16:], ("z", "y"), 1)
    near = [turned(message, "y", d) for d in (1, 2, 3)]

    def columns_for(chip):
        def cut(rows):
            mine = lax.dynamic_slice_in_dim(rows, chip * width + c * (width // 2), width // 2, 1)
            other = lax.dynamic_slice_in_dim(rows, chip * width + (1 - c) * (width // 2), width // 2, 1)
            return jnp.concatenate([mine, other], axis=1)

        return jnp.concatenate([cut(out_state), cut(out_conv)], axis=0)

    columns = [columns_for(x)] + [turned(columns_for((x + d) % chips), "x", d) for d in (1, 2, 3)]

    row_total, row_before, row_fade = join(row_kernel, "row", here_y, message, *near)
    far = [turned(row_total, "z", d) for d in (1, 2, 3)]
    conv_res = conv(
        first, normed, rim, gain_row, w_conv_h, w_conv_c, w_conv_b, conv_taps, group_gain.reshape(1, -1)
    )
    window, column_before, column_fade = join(column_kernel, "column", here_z, row_total, *far)
    farthest = turned(window, "z", 4)
    conv_all = [conv_res] + [turned(conv_res, "x", d) for d in (1, 2, 3)]
    reads, carries, gates = read(
        normed, w_query, w_outgate, state_gain.reshape(1, -1), keys, values, cums, starts, befores
    )
    state_res = finish(
        here_z, farthest, column_before, column_fade, row_before, row_fade, carries, reads, gates
    )
    state_all = [state_res] + [turned(state_res, "x", d) for d in (1, 2, 3)]
    half = project_half(conv_all, [w[F:] for w in columns])
    kept, sent = project_last(state_all, [w[:F] for w in columns], half)
    return (kept + turned(sent, "c", 1).astype(f32)).astype(bf16)


def solution(mesh):
    chips = 4
    rows = 4
    split = Mesh(
        mesh.devices.reshape(mesh.shape["sp"] // rows, rows, chips, mesh.shape["tp"] // chips),
        ("z", "y", "x", "c"),
    )
    sp, tp = ("z", "y"), ("x", "c")
    placed = (
        P(sp, None),
        P(),
        P(None, tp),
        P(None, tp),
        P(None, tp),
        P(None, tp),
        P(None, tp),
        P(None, tp),
        P(None, tp),
        P(tp),
        P(sp, tp),
        P(),
        P(None, tp),
        P(),
        P(tp, None),
        P(tp, None),
    )
    return jax.shard_map(body, mesh=split, in_specs=placed, out_specs=P(sp, tp), check_vma=False)
```

```python
import jax
import jax.numpy as jnp
from jax import lax
from jax.experimental import pallas as pl
from jax.experimental.pallas import tpu as pltpu
from jax.sharding import Mesh
from jax.sharding import PartitionSpec as P


F = 128
BLOCK = 64
TAPS = 3
STEP = 256
FRONT = 256
PACK = F + 16
EPS = 1e-06
f32 = jnp.float32
bf16 = jnp.bfloat16


def dot(a, b, dims=((1,), (0,))):
    return lax.dot_general(a, b, (dims, ((), ())), preferred_element_type=f32)


def rms(values, gain):
    return values * lax.rsqrt(jnp.mean(values * values, axis=-1, keepdims=True) + EPS) * gain


def silu(x):
    return x * jax.nn.sigmoid(x)


def put_message(ref, state, decay):
    high = decay.astype(bf16)
    low = (decay - high.astype(f32)).astype(bf16)
    ref[:F] = state.astype(bf16)
    row = lax.broadcasted_iota(jnp.int32, (16, F), 0)
    ref[F:] = jnp.where(row == 0, high.astype(f32), jnp.where(row == 1, low.astype(f32), 0.0)).astype(bf16)


def get_message(ref):
    tail = ref[F:].astype(f32)
    return ref[:F].astype(f32), tail[0:1] + tail[1:2]


def front_kernel(tokens, gain, w_forget, w_input, floor, leak,
                 normed, keys, values, cums, message,
                 weights, gates):
    step = pl.program_id(0)

    @pl.when(step == 0)
    def _():
        weights[:, :F] = w_forget[...]
        weights[:, F:] = w_input[...]

    n = rms(tokens[...].astype(f32), gain[...]).astype(bf16)
    normed[...] = n
    rows = pl.ds(pl.multiple_of(step * FRONT, FRONT), FRONT)
    gates[rows] = dot(n, weights[...]).astype(bf16)

    @pl.when(step == pl.num_programs(0) - 1)
    def _():
        row = lax.broadcasted_iota(jnp.int32, (STEP, STEP), 0)
        col = lax.broadcasted_iota(jnp.int32, (STEP, STEP), 1)
        tri = jnp.where(row >= col, 1.0, 0.0).astype(bf16)
        state = jnp.zeros((F, F), f32)
        total = jnp.zeros((1, F), f32)
        for at in range(0, gates.shape[0], STEP):
            value = gates[at : at + STEP, F:]
            values[at : at + STEP] = value
            gate = gates[at : at + STEP, :F].astype(f32)
            key = (1.0 - floor[...]) * jax.nn.sigmoid(-gate)
            keys[at : at + STEP] = key
            log_forget = jnp.log1p(-key) + leak[at : at + STEP]
            high = log_forget.astype(bf16)
            rest = log_forget - high.astype(f32)
            mid = rest.astype(bf16)
            low = (rest - mid.astype(f32)).astype(bf16)
            cum = dot(tri, high) + dot(tri, mid) + dot(tri, low)
            cums[at : at + STEP] = cum
            last = cum[STEP - 1 : STEP]
            fresh = dot(value, (key * jnp.exp(last - cum)).astype(bf16), ((0,), (0,)))
            state = state * jnp.exp(last) + fresh
            total = total + last
        put_message(message, state, jnp.exp(total))


def grant(mib, **more):
    return pltpu.CompilerParams(vmem_limit_bytes=mib * 2**20, **more)


def front(tokens, gain, w_forget, w_input, floor, leak):
    count, width = tokens.shape
    whole = lambda s: (0, 0)
    line = lambda s: (s, 0)
    return pl.pallas_call(
        front_kernel,
        grid=(count // FRONT,),
        in_specs=[
            pl.BlockSpec((FRONT, width), line),
            pl.BlockSpec((1, width), whole),
            pl.BlockSpec((width, F), whole),
            pl.BlockSpec((width, F), whole),
            pl.BlockSpec((1, F), whole),
            pl.BlockSpec((count, F), whole),
        ],
        out_specs=[
            pl.BlockSpec((FRONT, width), line),
            pl.BlockSpec((count, F), whole),
            pl.BlockSpec((count, F), whole),
            pl.BlockSpec((count, F), whole),
            pl.BlockSpec((PACK, F), whole),
        ],
        out_shape=[
            jax.ShapeDtypeStruct((count, width), bf16),
            jax.ShapeDtypeStruct((count, F), f32),
            jax.ShapeDtypeStruct((count, F), bf16),
            jax.ShapeDtypeStruct((count, F), f32),
            jax.ShapeDtypeStruct((PACK, F), bf16),
        ],
        scratch_shapes=[
            pltpu.VMEM((width, 2 * F), bf16),
            pltpu.VMEM((count, 2 * F), bf16),
        ],
        compiler_params=grant(60, dimension_semantics=("arbitrary",)),
        name="front",
    )(tokens, gain, w_forget, w_input, floor, leak)


def read_kernel(normed, w_query, w_outgate, gain, keys, values, cums,
                reads, carries, gates, weights, state, total):
    @pl.when(pl.program_id(0) == 0)
    def _():
        weights[:, :F] = w_query[...]
        weights[:, F:] = w_outgate[...]
        state[...] = jnp.zeros_like(state)
        total[...] = jnp.zeros_like(total)

    both = dot(normed[...], weights[...]).astype(bf16).astype(f32)
    query = silu(both[:, :F])
    gates[...] = silu(both[:, F:]) * gain[...]
    row = lax.broadcasted_iota(jnp.int32, (BLOCK, BLOCK), 0)
    col = lax.broadcasted_iota(jnp.int32, (BLOCK, BLOCK), 1)
    start = state[...]
    before = total[0:1]
    base = jnp.zeros((1, F), f32)
    for b in range(STEP // BLOCK):
        at = b * BLOCK
        q = query[at : at + BLOCK]
        k = keys[at : at + BLOCK]
        v = values[at : at + BLOCK]
        edge = cums[at + BLOCK - 1 : at + BLOCK]
        c = cums[at : at + BLOCK] - base
        half = c[BLOCK // 2 - 1 : BLOCK // 2]
        last = edge - base
        scores = dot((q * jnp.exp(c - half)).astype(bf16), (k * jnp.exp(half - c)).astype(bf16), ((1,), (1,)))
        scores = jnp.where(row >= col, scores, 0.0).astype(bf16)
        faded = q * jnp.exp(c)
        reads[at : at + BLOCK] = dot(scores, v) + dot(faded.astype(bf16), start.astype(bf16), ((1,), (1,)))
        carries[at : at + BLOCK] = (faded * jnp.exp(before + base)).astype(bf16)
        fresh = dot(v, (k * jnp.exp(last - c)).astype(bf16), ((0,), (0,)))
        start = start * jnp.exp(last) + fresh
        base = edge
    state[...] = start
    total[...] = jnp.broadcast_to(before + base, total.shape)


def read(normed, w_query, w_outgate, gain, keys, values, cums):
    count, width = normed.shape
    whole = lambda s: (0, 0)
    line = lambda s: (s, 0)
    return pl.pallas_call(
        read_kernel,
        grid=(count // STEP,),
        in_specs=[
            pl.BlockSpec((STEP, width), line),
            pl.BlockSpec((width, F), whole),
            pl.BlockSpec((width, F), whole),
            pl.BlockSpec((1, F), whole),
            pl.BlockSpec((STEP, F), line),
            pl.BlockSpec((STEP, F), line),
            pl.BlockSpec((STEP, F), line),
        ],
        out_specs=[pl.BlockSpec((STEP, F), line)] * 3,
        out_shape=[
            jax.ShapeDtypeStruct((count, F), f32),
            jax.ShapeDtypeStruct((count, F), bf16),
            jax.ShapeDtypeStruct((count, F), f32),
        ],
        scratch_shapes=[
            pltpu.VMEM((width, 2 * F), bf16),
            pltpu.VMEM((F, F), f32),
            pltpu.VMEM((8, F), f32),
        ],
        compiler_params=grant(16, dimension_semantics=("arbitrary",)),
        name="read",
    )(normed, w_query, w_outgate, gain, keys, values, cums)


def conv_kernel(first, normed, rim, in_gain, w_h, w_c, w_b, taps, gain, result, weights, window):
    step = pl.program_id(0)

    @pl.when(step == 0)
    def _():
        weights[:, :F] = w_h[...]
        weights[:, F:] = w_c[...]
        edge = rms(rim[...].astype(f32), in_gain[...]).astype(bf16)
        both = dot(edge, weights[...]).astype(bf16).astype(f32)
        signal = (both[:, :F] * both[:, F:]).astype(bf16).astype(f32)
        window[:8] = jnp.where(first[0] > 0, 0.0, signal[8:])

    @pl.when(step > 0)
    def _():
        window[:8] = window[STEP:]

    both = dot(normed[...], weights[...]).astype(bf16).astype(f32)
    window[8:] = (both[:, :F] * both[:, F:]).astype(bf16).astype(f32)
    scale = taps[...].astype(f32)
    total = scale[0:1] * window[6 : 6 + STEP]
    total = total + scale[1:2] * window[7 : 7 + STEP]
    total = total + scale[2:3] * window[8 : 8 + STEP]
    after = dot(normed[...], w_b[...]).astype(bf16).astype(f32)
    result[...] = rms(after * total, gain[...]).astype(bf16)


def conv(first, normed, rim, in_gain, w_h, w_c, w_b, taps, gain):
    count, width = normed.shape
    whole = lambda s: (0, 0)
    line = lambda s: (s, 0)
    return pl.pallas_call(
        conv_kernel,
        grid=(count // STEP,),
        in_specs=[
            pl.BlockSpec(memory_space=pltpu.SMEM),
            pl.BlockSpec((STEP, width), line),
            pl.BlockSpec((16, width), whole),
            pl.BlockSpec((1, width), whole),
            pl.BlockSpec((width, F), whole),
            pl.BlockSpec((width, F), whole),
            pl.BlockSpec((width, F), whole),
            pl.BlockSpec((TAPS, F), whole),
            pl.BlockSpec((1, F), whole),
        ],
        out_specs=pl.BlockSpec((STEP, F), line),
        out_shape=jax.ShapeDtypeStruct((count, F), bf16),
        scratch_shapes=[pltpu.VMEM((width, 2 * F), bf16), pltpu.VMEM((STEP + 8, F), f32)],
        compiler_params=grant(16, dimension_semantics=("arbitrary",)),
        name="conv",
    )(first, normed, rim, in_gain, w_h, w_c, w_b, taps, gain)


def row_kernel(index, own, one, two, three, total, before, fade):
    y = index[0]
    parts = [get_message(r) for r in (own, one, two, three)]
    place = [jnp.where(y >= d, y - d, y - d + 4) for d in range(4)]
    whole, inside = 0.0, 0.0
    product, product_before = 1.0, 1.0
    for d, (state, decay) in enumerate(parts):
        later = jnp.ones_like(decay)
        between = jnp.ones_like(decay)
        for other, (_, factor) in enumerate(parts):
            if other == d:
                continue
            behind = place[other] > place[d]
            later = later * jnp.where(behind, factor, 1.0)
            between = between * jnp.where(behind & (place[other] < y), factor, 1.0)
        whole = whole + state * later
        inside = inside + state * jnp.where(place[d] < y, between, 0.0)
        product = product * decay
        product_before = product_before * jnp.where(place[d] < y, decay, 1.0)
    put_message(total, whole, product)
    before[...] = inside
    fade[...] = jnp.broadcast_to(product_before, fade.shape)


def column_kernel(index, own, one, two, three, window, before, fade):
    z = index[0]
    state, product = jnp.zeros((F, F), f32), jnp.ones((1, F), f32)
    for d, ref in ((3, three), (2, two), (1, one)):
        piece, decay = get_message(ref)
        decay = jnp.where(z >= d, decay, 1.0)
        state = state * decay + jnp.where(z >= d, piece, 0.0)
        product = product * decay
    piece, decay = get_message(own)
    put_message(window, state * decay + piece, product * decay)
    before[...] = state
    fade[...] = jnp.broadcast_to(product, fade.shape)


def join(kernel, index, *messages):
    vmem = pl.BlockSpec(memory_space=pltpu.VMEM)
    return pl.pallas_call(
        kernel,
        in_specs=[pl.BlockSpec(memory_space=pltpu.SMEM)] + [vmem] * 4,
        out_specs=[vmem] * 3,
        out_shape=[
            jax.ShapeDtypeStruct((PACK, F), bf16),
            jax.ShapeDtypeStruct((F, F), f32),
            jax.ShapeDtypeStruct((8, F), f32),
        ],
        compiler_params=grant(4),
    )(index, *messages)


def finish_kernel(index, far, column, column_fade, row, row_fade, carries, reads, gates, result):
    piece, _ = get_message(far)
    piece = jnp.where(index[0] >= 4, piece, 0.0)
    incoming = (column[...] + piece * column_fade[0:1]) * row_fade[0:1] + row[...]
    found = reads[...] + dot(carries[...], incoming.astype(bf16), ((1,), (1,)))
    result[...] = rms(found, gates[...]).astype(bf16)


def finish(index, far, column, column_fade, row, row_fade, carries, reads, gates):
    vmem = pl.BlockSpec(memory_space=pltpu.VMEM)
    return pl.pallas_call(
        finish_kernel,
        in_specs=[pl.BlockSpec(memory_space=pltpu.SMEM)] + [vmem] * 8,
        out_specs=vmem,
        out_shape=jax.ShapeDtypeStruct(reads.shape, bf16),
        compiler_params=grant(12),
        name="finish",
    )(index, far, column, column_fade, row, row_fade, carries, reads, gates)


def half_kernel(*refs):
    parts, weights, out = refs[:4], refs[4:8], refs[8]
    out[...] = dot(
        jnp.concatenate([r[...] for r in parts], axis=1),
        jnp.concatenate([r[F:] for r in weights], axis=0),
    )


def last_kernel(*refs):
    parts, weights, earlier, kept, sent = refs[:4], refs[4:8], refs[8], refs[9], refs[10]
    total = earlier[...] + dot(
        jnp.concatenate([r[...] for r in parts], axis=1),
        jnp.concatenate([r[:F] for r in weights], axis=0),
    )
    width = total.shape[1] // 2
    kept[...] = total[:, :width]
    sent[...] = total[:, width:].astype(bf16)


def project_half(parts, weights):
    vmem = pl.BlockSpec(memory_space=pltpu.VMEM)
    return pl.pallas_call(
        half_kernel,
        in_specs=[vmem] * 8,
        out_specs=vmem,
        out_shape=jax.ShapeDtypeStruct((parts[0].shape[0], weights[0].shape[1]), f32),
        compiler_params=grant(16),
        name="half",
    )(*parts, *weights)


def project_last(parts, weights, earlier):
    vmem = pl.BlockSpec(memory_space=pltpu.VMEM)
    count, width = earlier.shape
    return pl.pallas_call(
        last_kernel,
        in_specs=[vmem] * 9,
        out_specs=[vmem] * 2,
        out_shape=[
            jax.ShapeDtypeStruct((count, width // 2), f32),
            jax.ShapeDtypeStruct((count, width // 2), bf16),
        ],
        compiler_params=grant(16),
        name="last",
    )(*parts, *weights, earlier)


def turned(array, axis, by):
    count = lax.axis_size(axis)
    return lax.ppermute(array, axis, [(i, (i + by) % count) for i in range(count)])


def body(
    tokens,
    in_gain,
    w_query,
    w_forget,
    w_input,
    w_outgate,
    w_conv_h,
    w_conv_b,
    w_conv_c,
    forget_floor,
    forget_leak,
    state_gain,
    conv_taps,
    group_gain,
    out_state,
    out_conv,
):
    x, c = lax.axis_index("x"), lax.axis_index("c")
    y, z = lax.axis_index("y"), lax.axis_index("z")
    here_y = y.astype(jnp.int32).reshape(1)
    here_z = z.astype(jnp.int32).reshape(1)
    first = ((y == 0) & (z == 0)).astype(jnp.int32).reshape(1)
    chips = lax.axis_size("x")
    width = tokens.shape[1] // chips
    gain_row = in_gain.reshape(1, -1)

    normed, keys, values, cums, message = front(
        tokens, gain_row, w_forget, w_input, forget_floor.reshape(1, -1), forget_leak
    )
    rim = turned(tokens[-16:], ("z", "y"), 1)
    near = [turned(message, "y", d) for d in (1, 2, 3)]

    def columns_for(chip):
        def cut(rows):
            mine = lax.dynamic_slice_in_dim(rows, chip * width + c * (width // 2), width // 2, 1)
            other = lax.dynamic_slice_in_dim(rows, chip * width + (1 - c) * (width // 2), width // 2, 1)
            return jnp.concatenate([mine, other], axis=1)

        return jnp.concatenate([cut(out_state), cut(out_conv)], axis=0)

    columns = [columns_for(x)] + [turned(columns_for((x + d) % chips), "x", d) for d in (1, 2, 3)]

    row_total, row_before, row_fade = join(row_kernel, here_y, message, *near)
    far = [turned(row_total, "z", d) for d in (1, 2, 3)]
    conv_res = conv(
        first, normed, rim, gain_row, w_conv_h, w_conv_c, w_conv_b, conv_taps, group_gain.reshape(1, -1)
    )
    window, column_before, column_fade = join(column_kernel, here_z, row_total, *far)
    farthest = turned(window, "z", 4)
    conv_all = [conv_res] + [turned(conv_res, "x", d) for d in (1, 2, 3)]
    reads, carries, gates = read(
        normed, w_query, w_outgate, state_gain.reshape(1, -1), keys, values, cums
    )
    state_res = finish(
        here_z, farthest, column_before, column_fade, row_before, row_fade, carries, reads, gates
    )
    state_all = [state_res] + [turned(state_res, "x", d) for d in (1, 2, 3)]
    half = project_half(conv_all, columns)
    kept, sent = project_last(state_all, columns, half)
    return (kept + turned(sent, "c", 1).astype(f32)).astype(bf16)


def solution(mesh):
    chips = 4
    rows = 4
    split = Mesh(
        mesh.devices.reshape(mesh.shape["sp"] // rows, rows, chips, mesh.shape["tp"] // chips),
        ("z", "y", "x", "c"),
    )
    sp, tp = ("z", "y"), ("x", "c")
    placed = (
        P(sp, None),
        P(),
        P(None, tp),
        P(None, tp),
        P(None, tp),
        P(None, tp),
        P(None, tp),
        P(None, tp),
        P(None, tp),
        P(tp),
        P(sp, tp),
        P(),
        P(None, tp),
        P(),
        P(tp, None),
        P(tp, None),
    )
    return jax.shard_map(body, mesh=split, in_specs=placed, out_specs=P(sp, tp), check_vma=False)
```

```python
import jax
import jax.numpy as jnp
from jax import lax
from jax.experimental import pallas as pl
from jax.experimental.pallas import tpu as pltpu
from jax.sharding import Mesh
from jax.sharding import PartitionSpec as P


F = 128
BLOCK = 64
TAPS = 3
STEP = 256
FRONT = 256
PACK = F + 16
EPS = 1e-06
f32 = jnp.float32
bf16 = jnp.bfloat16


def dot(a, b, dims=((1,), (0,))):
    return lax.dot_general(a, b, (dims, ((), ())), preferred_element_type=f32)


def rms(values, gain):
    return values * lax.rsqrt(jnp.mean(values * values, axis=-1, keepdims=True) + EPS) * gain


def silu(x):
    return x * jax.nn.sigmoid(x)


def put_message(ref, state, decay, rim):
    high = decay.astype(bf16)
    low = (decay - high.astype(f32)).astype(bf16)
    ref[:F] = state.astype(bf16)
    row = lax.broadcasted_iota(jnp.int32, (16, F), 0)
    tail = jnp.where(row == 0, high.astype(f32), jnp.where(row == 1, low.astype(f32), 0.0))
    tail = jnp.where(row == 2, rim[0:1], jnp.where(row == 3, rim[1:2], tail))
    ref[F:] = tail.astype(bf16)


def get_message(ref):
    tail = ref[F:].astype(f32)
    return ref[:F].astype(f32), tail[0:1] + tail[1:2]


def get_rim(ref):
    return ref[F:].astype(f32)[2:4]


def grant(mib, **more):
    return pltpu.CompilerParams(vmem_limit_bytes=mib * 2**20, **more)


def front_kernel(place, tokens_h, gain_h, wf_h, wi_h, wq_h, wg_h, wh_h, wc_h, wb_h, floor_h, leak_h,
                 taps_h, group_h, sgain_h, ostate_h, oconv_h,
                 message, keys, values, cums, heads, extra, own, one, two, three,
                 tokens, gain, weights, floor, leak, taps, group, sgain, ostate, oconv, window, sems):
    count = tokens.shape[0]
    width = ostate.shape[1]
    copies = []

    def bring(src, dst):
        copy = pltpu.make_async_copy(src, dst, sems.at[len(copies)])
        copy.start()
        copies.append(copy)
        return copy

    def rows(step):
        return pl.ds(step * FRONT, FRONT)

    got_gain = bring(gain_h, gain)
    got_tokens = [bring(tokens_h.at[rows(0)], tokens.at[rows(0)])]
    got_weights = [
        bring(w, weights.at[:, pl.ds(j * F, F)])
        for j, w in enumerate((wf_h, wi_h, wq_h, wg_h, wh_h, wc_h, wb_h))
    ]
    small = [bring(floor_h, floor), bring(leak_h, leak), bring(taps_h, taps), bring(group_h, group), bring(sgain_h, sgain)]
    for step in range(1, count // FRONT):
        got_tokens.append(bring(tokens_h.at[rows(step)], tokens.at[rows(step)]))
    last_copies = [bring(ostate_h, ostate), bring(oconv_h, oconv)]

    row = lax.broadcasted_iota(jnp.int32, (STEP, STEP), 0)
    col = lax.broadcasted_iota(jnp.int32, (STEP, STEP), 1)
    tri = jnp.where(row >= col, 1.0, 0.0).astype(bf16)
    state = jnp.zeros((F, F), f32)
    total = jnp.zeros((1, F), f32)
    window[:8] = jnp.zeros((8, F), f32)
    got_gain.wait()
    for step in range(count // FRONT):
        top = step * FRONT
        got_tokens[step].wait()
        n = rms(tokens[top : top + FRONT].astype(f32), gain[...]).astype(bf16)
        if step == 0:
            for copy in got_weights:
                copy.wait()
        found = dot(n, weights[...]).astype(bf16)
        if step == 0:
            for copy in small:
                copy.wait()
        value = found[:, F : 2 * F]
        values[top : top + FRONT] = value
        heads[top : top + FRONT] = found[:, 2 * F : 4 * F]
        gate = found[:, :F].astype(f32)
        key = (1.0 - floor[...]) * jax.nn.sigmoid(-gate)
        keys[top : top + FRONT] = key
        log_forget = jnp.log1p(-key) + leak[top : top + FRONT]
        high = log_forget.astype(bf16)
        rest = log_forget - high.astype(f32)
        mid = rest.astype(bf16)
        low = (rest - mid.astype(f32)).astype(bf16)
        for at in range(0, FRONT, STEP):
            part = slice(at, at + STEP)
            cum = dot(tri, high[part]) + dot(tri, mid[part]) + dot(tri, low[part])
            cums[top + at : top + at + STEP] = cum
            last = cum[STEP - 1 : STEP]
            fresh = dot(value[part], (key[part] * jnp.exp(last - cum)).astype(bf16), ((0,), (0,)))
            state = state * jnp.exp(last) + fresh
            total = total + last
        signal = (found[:, 4 * F : 5 * F].astype(f32) * found[:, 5 * F : 6 * F].astype(f32)).astype(bf16).astype(f32)
        window[8 + top : 8 + top + FRONT] = signal
        scale = taps[...].astype(f32)
        near = scale[0:1] * window[6 + top : 6 + top + FRONT]
        near = near + scale[1:2] * window[7 + top : 7 + top + FRONT]
        near = near + scale[2:3] * signal
        after = found[:, 6 * F :].astype(f32)
        result = rms(after * near, group[...]).astype(bf16)
        for buffer in (own, one, two, three):
            buffer[top : top + FRONT] = result
        if step == 0:
            extra[:16] = signal[:16]
            extra[16:32] = after[:16]
            extra[32:35] = scale
            extra[35:36] = group[...]
            extra[36:37] = sgain[...]
    put_message(message, state, jnp.exp(total), window[count + 6 : count + 8])
    for copy in last_copies:
        copy.wait()
    _, _, x, c = unpack_place(place)
    for d, buffer in enumerate((own, one, two, three)):
        chip = (x + d) & 3
        for j in range(4):
            core = c if j < 2 else 1 - c
            at = pl.multiple_of(chip * (width // 4) + core * (width // 8) + (j & 1) * F, F)
            buffer[count + 2 * j * F : count + (2 * j + 1) * F] = ostate[:, pl.ds(at, F)]
            buffer[count + (2 * j + 1) * F : count + (2 * j + 2) * F] = oconv[:, pl.ds(at, F)]


def unpack_place(place):
    code = place[0]
    return code >> 5, (code >> 3) & 3, (code >> 1) & 3, code & 1


def front(place, tokens, gain, w7, floor, leak, taps, group, sgain, ostate, oconv):
    count, width = tokens.shape
    hbm = pl.BlockSpec(memory_space=pltpu.HBM)
    vmem = pl.BlockSpec(memory_space=pltpu.VMEM)
    buffer = jax.ShapeDtypeStruct((count + 8 * F, F), bf16)
    arrays = (tokens, gain, *w7, floor, leak, taps, group, sgain, ostate, oconv)
    return pl.pallas_call(
        front_kernel,
        in_specs=[pl.BlockSpec(memory_space=pltpu.SMEM)] + [hbm] * len(arrays),
        out_specs=[vmem] * 10,
        out_shape=[
            jax.ShapeDtypeStruct((PACK, F), bf16),
            jax.ShapeDtypeStruct((count, F), f32),
            jax.ShapeDtypeStruct((count, F), bf16),
            jax.ShapeDtypeStruct((count, F), f32),
            jax.ShapeDtypeStruct((count, 2 * F), bf16),
            jax.ShapeDtypeStruct((40, F), f32),
        ]
        + [buffer] * 4,
        scratch_shapes=[
            pltpu.VMEM((count, width), bf16),
            pltpu.VMEM((1, width), f32),
            pltpu.VMEM((width, 7 * F), bf16),
            pltpu.VMEM((1, F), f32),
            pltpu.VMEM((count, F), f32),
            pltpu.VMEM((TAPS, F), bf16),
            pltpu.VMEM((1, F), f32),
            pltpu.VMEM((1, F), f32),
            pltpu.VMEM(ostate.shape, bf16),
            pltpu.VMEM(oconv.shape, bf16),
            pltpu.VMEM((count + 8, F), f32),
            pltpu.SemaphoreType.DMA((15 + count // FRONT,)),
        ],
        compiler_params=grant(36),
        name="front",
    )(place, *[pltpu.with_memory_space_constraint(a, pltpu.HBM) for a in arrays])


def read_kernel(heads, extra, keys, values, cums, reads, carries, gates):
    row = lax.broadcasted_iota(jnp.int32, (BLOCK, BLOCK), 0)
    col = lax.broadcasted_iota(jnp.int32, (BLOCK, BLOCK), 1)
    start = jnp.zeros((F, F), f32)
    before = jnp.zeros((1, F), f32)
    for at in range(0, heads.shape[0], BLOCK):
        part = slice(at, at + BLOCK)
        gates[part] = silu(heads[part, F:].astype(f32)) * extra[36:37]
        q = silu(heads[part, :F].astype(f32))
        k = keys[part]
        v = values[part]
        base = jnp.zeros((1, F), f32) if at % STEP == 0 else cums[at - 1 : at]
        edge = cums[at + BLOCK - 1 : at + BLOCK]
        c = cums[part] - base
        half = c[BLOCK // 2 - 1 : BLOCK // 2]
        last = edge - base
        scores = dot((q * jnp.exp(c - half)).astype(bf16), (k * jnp.exp(half - c)).astype(bf16), ((1,), (1,)))
        scores = jnp.where(row >= col, scores, 0.0).astype(bf16)
        faded = q * jnp.exp(c)
        reads[part] = dot(scores, v) + dot(faded.astype(bf16), start.astype(bf16), ((1,), (1,)))
        carries[part] = (faded * jnp.exp(before)).astype(bf16)
        fresh = dot(v, (k * jnp.exp(last - c)).astype(bf16), ((0,), (0,)))
        start = start * jnp.exp(last) + fresh
        before = before + last


def read(heads, extra, keys, values, cums):
    count = heads.shape[0]
    vmem = pl.BlockSpec(memory_space=pltpu.VMEM)
    return pl.pallas_call(
        read_kernel,
        in_specs=[vmem] * 5,
        out_specs=[vmem] * 3,
        out_shape=[
            jax.ShapeDtypeStruct((count, F), f32),
            jax.ShapeDtypeStruct((count, F), bf16),
            jax.ShapeDtypeStruct((count, F), f32),
        ],
        compiler_params=grant(12),
        name="read",
    )(heads, extra, keys, values, cums)


def row_kernel(place_ref, own, one, two, three, total, before, fade):
    _, y, _, _ = unpack_place(place_ref)
    parts = [get_message(r) for r in (own, one, two, three)]
    place = [jnp.where(y >= d, y - d, y - d + 4) for d in range(4)]
    whole, inside = 0.0, 0.0
    product, product_before = 1.0, 1.0
    for d, (state, decay) in enumerate(parts):
        later = jnp.ones_like(decay)
        between = jnp.ones_like(decay)
        for other, (_, factor) in enumerate(parts):
            if other == d:
                continue
            behind = place[other] > place[d]
            later = later * jnp.where(behind, factor, 1.0)
            between = between * jnp.where(behind & (place[other] < y), factor, 1.0)
        whole = whole + state * later
        inside = inside + state * jnp.where(place[d] < y, between, 0.0)
        product = product * decay
        product_before = product_before * jnp.where(place[d] < y, decay, 1.0)
    put_message(total, whole, product, get_rim(one))
    before[...] = inside
    fade[...] = jnp.broadcast_to(product_before, fade.shape)


def column_kernel(place_ref, own, one, two, three, window, before, fade):
    z, _, _, _ = unpack_place(place_ref)
    state, product = jnp.zeros((F, F), f32), jnp.ones((1, F), f32)
    for d, ref in ((3, three), (2, two), (1, one)):
        piece, decay = get_message(ref)
        decay = jnp.where(z >= d, decay, 1.0)
        state = state * decay + jnp.where(z >= d, piece, 0.0)
        product = product * decay
    piece, decay = get_message(own)
    put_message(window, state * decay + piece, product * decay, get_rim(one))
    before[...] = state
    fade[...] = jnp.broadcast_to(product, fade.shape)


def join(kernel, index, *messages):
    vmem = pl.BlockSpec(memory_space=pltpu.VMEM)
    return pl.pallas_call(
        kernel,
        in_specs=[pl.BlockSpec(memory_space=pltpu.SMEM)] + [vmem] * 4,
        out_specs=[vmem] * 3,
        out_shape=[
            jax.ShapeDtypeStruct((PACK, F), bf16),
            jax.ShapeDtypeStruct((F, F), f32),
            jax.ShapeDtypeStruct((8, F), f32),
        ],
        compiler_params=grant(4),
    )(index, *messages)


def finish_kernel(place, far, near, row_total, column, column_fade, row, row_fade, carries, reads, gates, extra,
                  result, window):
    z, y, _, _ = unpack_place(place)
    piece, _ = get_message(far)
    piece = jnp.where(z >= 4, piece, 0.0)
    incoming = (column[...] + piece * column_fade[0:1]) * row_fade[0:1] + row[...]
    count = reads.shape[0]
    found = reads[...] + dot(carries[...], incoming.astype(bf16), ((1,), (1,)))
    result[:count] = rms(found, gates[...]).astype(bf16)
    rim = jnp.where(y > 0, get_rim(row_total), jnp.where(z > 0, get_rim(near), 0.0))
    window[6:8] = rim
    window[8:] = extra[:16]
    total = extra[32:33] * window[6:22] + extra[33:34] * window[7:23] + extra[34:35] * window[8:24]
    result[count:] = rms(extra[16:32] * total, extra[35:36]).astype(bf16)


def finish(place, *arrays):
    vmem = pl.BlockSpec(memory_space=pltpu.VMEM)
    return pl.pallas_call(
        finish_kernel,
        in_specs=[pl.BlockSpec(memory_space=pltpu.SMEM)] + [vmem] * len(arrays),
        out_specs=vmem,
        out_shape=jax.ShapeDtypeStruct((arrays[8].shape[0] + 16, F), bf16),
        scratch_shapes=[pltpu.VMEM((24, F), f32)],
        compiler_params=grant(12),
        name="finish",
    )(place, *arrays)


def weight_rows(buffers, half):
    count = buffers[0].shape[0] - 8 * F
    at = [count + (2 * j + half) * F for j in range(4)]
    return jnp.concatenate(
        [jnp.concatenate([r[a : a + F] for a in at], axis=1) for r in buffers], axis=0
    )


def half_kernel(own, one, two, three, out):
    buffers = (own, one, two, three)
    count = out.shape[0]
    out[...] = dot(jnp.concatenate([r[:count] for r in buffers], axis=1), weight_rows(buffers, 1))


def last_kernel(*refs):
    parts, buffers, earlier, kept, sent = refs[:4], refs[4:8], refs[8], refs[9], refs[10]
    count, full = earlier.shape
    width = full // 2
    state = dot(jnp.concatenate([r[:count] for r in parts], axis=1), weight_rows(buffers, 0))
    total = earlier[...] + state
    kept[...] = total[:, :width]
    sent[...] = total[:, width:].astype(bf16)
    first = state[:16] + dot(jnp.concatenate([r[count:] for r in parts], axis=1), weight_rows(buffers, 1))
    kept[:16] = first[:, :width]
    sent[:16] = first[:, width:].astype(bf16)


def project_half(buffers):
    vmem = pl.BlockSpec(memory_space=pltpu.VMEM)
    return pl.pallas_call(
        half_kernel,
        in_specs=[vmem] * 4,
        out_specs=vmem,
        out_shape=jax.ShapeDtypeStruct((buffers[0].shape[0] - 8 * F, 4 * F), f32),
        compiler_params=grant(14),
        name="half",
    )(*buffers)


def project_last(parts, buffers, earlier):
    vmem = pl.BlockSpec(memory_space=pltpu.VMEM)
    count, width = earlier.shape
    return pl.pallas_call(
        last_kernel,
        in_specs=[vmem] * 9,
        out_specs=[vmem] * 2,
        out_shape=[
            jax.ShapeDtypeStruct((count, width // 2), f32),
            jax.ShapeDtypeStruct((count, width // 2), bf16),
        ],
        compiler_params=grant(16),
        name="last",
    )(*parts, *buffers, earlier)


def turned(array, axis, by):
    count = lax.axis_size(axis)
    return lax.ppermute(array, axis, [(i, (i + by) % count) for i in range(count)])


def body(
    tokens,
    in_gain,
    w_query,
    w_forget,
    w_input,
    w_outgate,
    w_conv_h,
    w_conv_b,
    w_conv_c,
    forget_floor,
    forget_leak,
    state_gain,
    conv_taps,
    group_gain,
    out_state,
    out_conv,
):
    code = (lax.axis_index("z") * 4 + lax.axis_index("y")) * 4 + lax.axis_index("x")
    place = (code * 2 + lax.axis_index("c")).astype(jnp.int32).reshape(1)
    line = lambda row: row.reshape(1, -1)
    message, keys, values, cums, heads, extra, *buffers = front(
        place,
        tokens,
        line(in_gain),
        (w_forget, w_input, w_query, w_outgate, w_conv_h, w_conv_c, w_conv_b),
        line(forget_floor),
        forget_leak,
        conv_taps,
        line(group_gain),
        line(state_gain),
        out_state,
        out_conv,
    )
    near = [turned(message, "y", d) for d in (1, 2, 3)]
    buffers = buffers[:1] + [turned(buffers[d], "x", d) for d in (1, 2, 3)]
    row_total, row_before, row_fade = join(row_kernel, place, message, *near)
    far = [turned(row_total, "z", d) for d in (1, 2, 3)]
    reads, carries, gates = read(heads, extra, keys, values, cums)
    window, column_before, column_fade = join(column_kernel, place, row_total, *far)
    farthest = turned(window, "z", 4)
    state_res = finish(
        place, farthest, far[0], row_total, column_before, column_fade, row_before, row_fade,
        carries, reads, gates, extra,
    )
    state_all = [state_res] + [turned(state_res, "x", d) for d in (1, 2, 3)]
    half = project_half(buffers)
    kept, sent = project_last(state_all, buffers, half)
    return (kept + turned(sent, "c", 1).astype(f32)).astype(bf16)


def solution(mesh):
    chips = 4
    rows = 4
    split = Mesh(
        mesh.devices.reshape(mesh.shape["sp"] // rows, rows, chips, mesh.shape["tp"] // chips),
        ("z", "y", "x", "c"),
    )
    sp, tp = ("z", "y"), ("x", "c")
    placed = (
        P(sp, None),
        P(),
        P(None, tp),
        P(None, tp),
        P(None, tp),
        P(None, tp),
        P(None, tp),
        P(None, tp),
        P(None, tp),
        P(tp),
        P(sp, tp),
        P(),
        P(None, tp),
        P(),
        P(tp, None),
        P(tp, None),
    )
    return jax.shard_map(body, mesh=split, in_specs=placed, out_specs=P(sp, tp), check_vma=False)
```

```python
import functools

import jax
import jax.numpy as jnp
from jax import lax
from jax.experimental import pallas as pl
from jax.experimental.pallas import tpu as pltpu
from jax.sharding import Mesh
from jax.sharding import PartitionSpec as P


F = 128
BLOCK = 64
STEP = 256
FRONT = 256
PACK = F + 16
EPS = 1e-06
ROWS = 8
f32 = jnp.float32
bf16 = jnp.bfloat16


def dot(a, b, dims=((1,), (0,))):
    return lax.dot_general(a, b, (dims, ((), ())), preferred_element_type=f32)


def rms(values, gain):
    return values * lax.rsqrt(jnp.mean(values * values, axis=-1, keepdims=True) + EPS) * gain


def silu(x):
    return x * jax.nn.sigmoid(x)


def put_message(ref, state, decay, rim):
    high = decay.astype(bf16)
    low = (decay - high.astype(f32)).astype(bf16)
    ref[:F] = state.astype(bf16)
    row = lax.broadcasted_iota(jnp.int32, (16, F), 0)
    tail = jnp.where(row == 0, high.astype(f32), jnp.where(row == 1, low.astype(f32), 0.0))
    tail = jnp.where(row == 2, rim[0:1], jnp.where(row == 3, rim[1:2], tail))
    ref[F:] = tail.astype(bf16)


def get_message(ref):
    tail = ref[F:].astype(f32)
    return ref[:F].astype(f32), tail[0:1] + tail[1:2]


def get_rim(ref):
    return ref[F:].astype(f32)[2:4]


def grant(mib, **more):
    return pltpu.CompilerParams(vmem_limit_bytes=mib * 2**20, **more)


def front_kernel(place, tokens_h, gain_h, wf_h, wi_h, wh_h, wc_h, wb_h, wq_h, wg_h, floor_h, leak_h,
                 ostate_h, oconv_h,
                 tokens, scales, message, keys, values, cums, later, own, one, two, three,
                 gain, weights, floor, leak, ostate, oconv, sems):
    count, width = tokens.shape
    copies = []

    def bring(src, dst):
        copy = pltpu.make_async_copy(src, dst, sems.at[len(copies)])
        copy.start()
        copies.append(copy)
        return copy

    got_gain = bring(gain_h, gain)
    half = FRONT // 2
    got_first = [bring(tokens_h.at[pl.ds(at, half)], tokens.at[pl.ds(at, half)]) for at in (0, half)]
    got_weights = [bring(w, weights.at[:, pl.ds(j * F, F)]) for j, w in enumerate((wf_h, wi_h))]
    others = [bring(floor_h, floor), bring(leak_h, leak)]
    others += [
        bring(tokens_h.at[pl.ds(at, FRONT)], tokens.at[pl.ds(at, FRONT)]) for at in range(FRONT, count, FRONT)
    ]
    last_copies = [bring(wh_h, later.at[:, pl.ds(0, F)]), bring(wc_h, later.at[:, pl.ds(F, F)])]
    last_copies += [bring(ostate_h, ostate), bring(oconv_h, oconv)]
    next_copies = [bring(w, later.at[:, pl.ds((2 + j) * F, F)]) for j, w in enumerate((wb_h, wq_h, wg_h))]

    row = lax.broadcasted_iota(jnp.int32, (STEP, STEP), 0)
    col = lax.broadcasted_iota(jnp.int32, (STEP, STEP), 1)
    tri = jnp.where(row >= col, 1.0, 0.0).astype(bf16)
    state = jnp.zeros((F, F), f32)
    total = jnp.zeros((1, F), f32)

    def norm(top, size):
        part = tokens[top : top + size].astype(f32)
        mean = jnp.mean(part * part, axis=-1, keepdims=True)
        scales[top : top + size] = jnp.broadcast_to(lax.rsqrt(mean + EPS), (size, F))
        tokens[top : top + size] = (part * gain[...]).astype(bf16)

    def project(top):
        scale = scales[top : top + FRONT]
        found = dot(tokens[top : top + FRONT], weights[...])
        return (found * jnp.concatenate([scale, scale], axis=1)).astype(bf16)

    def gates(top, found, state, total):
        value = found[:, F:]
        values[top : top + FRONT] = value
        gate = found[:, :F].astype(f32)
        key = (1.0 - floor[...]) * jax.nn.sigmoid(-gate)
        keys[top : top + FRONT] = key
        log_forget = jnp.log1p(-key) + leak[top : top + FRONT]
        high = log_forget.astype(bf16)
        rest = log_forget - high.astype(f32)
        mid = rest.astype(bf16)
        low = (rest - mid.astype(f32)).astype(bf16)
        for at in range(0, FRONT, STEP):
            part = slice(at, at + STEP)
            cum = dot(tri, high[part]) + dot(tri, mid[part]) + dot(tri, low[part])
            cums[top + at : top + at + STEP] = cum
            last = cum[STEP - 1 : STEP]
            fresh = dot(value[part], (key[part] * jnp.exp(last - cum)).astype(bf16), ((0,), (0,)))
            state = state * jnp.exp(last) + fresh
            total = total + last
        return state, total

    got_gain.wait()
    for copy, top in zip(got_first, (0, half)):
        copy.wait()
        norm(top, half)
    for copy in got_weights:
        copy.wait()
    found = project(0)
    for copy in others:
        copy.wait()
    for top in range(FRONT, count, FRONT):
        norm(top, FRONT)
        following = project(top)
        state, total = gates(top - FRONT, found, state, total)
        found = following
    for copy in last_copies:
        copy.wait()
    scale = scales[count - 16 :]
    edge = dot(tokens[count - 16 :], later[:, : 2 * F]) * jnp.concatenate([scale, scale], axis=1)
    edge = edge.astype(bf16).astype(f32)
    state, total = gates(count - FRONT, found, state, total)
    put_message(message, state, jnp.exp(total), (edge[:, :F] * edge[:, F:])[14:])
    _, _, x, c = unpack_place(place)
    for d, buffer in enumerate((own, one, two, three)):
        for j in range(4):
            core = c if j < 2 else 1 - c
            at = pl.multiple_of(((x + d) & 3) * (width // 4) + core * (width // 8) + (j & 1) * F, F)
            buffer[:F, j * F : (j + 1) * F] = ostate[:, pl.ds(at, F)]
            buffer[F:, j * F : (j + 1) * F] = oconv[:, pl.ds(at, F)]
    for copy in next_copies:
        copy.wait()


def unpack_place(place):
    code = place[0]
    return code >> 5, (code >> 3) & 3, (code >> 1) & 3, code & 1


def in_hbm(arrays):
    return [pltpu.with_memory_space_constraint(a, pltpu.HBM) for a in arrays]


def front(place, *arrays):
    count, width = arrays[0].shape
    ostate = arrays[-1]
    hbm = pl.BlockSpec(memory_space=pltpu.HBM)
    vmem = pl.BlockSpec(memory_space=pltpu.VMEM)
    return pl.pallas_call(
        front_kernel,
        in_specs=[pl.BlockSpec(memory_space=pltpu.SMEM)] + [hbm] * len(arrays),
        out_specs=[vmem] * 11,
        out_shape=[
            jax.ShapeDtypeStruct((count, width), bf16),
            jax.ShapeDtypeStruct((count, F), f32),
            jax.ShapeDtypeStruct((PACK, F), bf16),
            jax.ShapeDtypeStruct((count, F), f32),
            jax.ShapeDtypeStruct((count, F), bf16),
            jax.ShapeDtypeStruct((count, F), f32),
            jax.ShapeDtypeStruct((width, 5 * F), bf16),
        ]
        + [jax.ShapeDtypeStruct((2 * F, 4 * F), bf16)] * 4,
        scratch_shapes=[
            pltpu.VMEM((1, width), f32),
            pltpu.VMEM((width, 2 * F), bf16),
            pltpu.VMEM((1, F), f32),
            pltpu.VMEM((count, F), f32),
            pltpu.VMEM(ostate.shape, bf16),
            pltpu.VMEM(ostate.shape, bf16),
            pltpu.SemaphoreType.DMA((13 + count // FRONT,)),
        ],
        compiler_params=grant(24),
        name="front",
    )(place, *in_hbm(arrays))


def conv_kernel(normed, scales, weights, taps, group, sgain, heads, extra, result, window):
    count = normed.shape[0]
    window[:8] = jnp.zeros((8, F), f32)

    def project(top, first, last):
        found = dot(normed[top : top + FRONT], weights[:, first * F : last * F])
        return (found * jnp.concatenate([scales[top : top + FRONT]] * (last - first), axis=1)).astype(bf16)

    def convolve(top, found):
        signal = (found[:, :F].astype(f32) * found[:, F : 2 * F].astype(f32)).astype(bf16).astype(f32)
        window[8 + top : 8 + top + FRONT] = signal
        scale = taps[...].astype(f32)
        near = scale[0:1] * window[6 + top : 6 + top + FRONT]
        near = near + scale[1:2] * window[7 + top : 7 + top + FRONT]
        near = near + scale[2:3] * signal
        after = found[:, 2 * F :].astype(f32)
        result[top : top + FRONT] = rms(after * near, group[...]).astype(bf16)
        if top == 0:
            extra[:16] = signal[:16]
            extra[16:32] = after[:16]
            extra[32:35] = scale
            extra[35:36] = group[...]
            extra[36:37] = sgain[...]

    for top in range(0, count, FRONT):
        mixed = project(top, 0, 3)
        heads[top : top + FRONT] = project(top, 3, 5)
        convolve(top, mixed)


def conv(normed, *arrays):
    count, _ = normed.shape
    vmem = pl.BlockSpec(memory_space=pltpu.VMEM)
    return pl.pallas_call(
        conv_kernel,
        in_specs=[vmem] * 6,
        out_specs=[vmem] * 3,
        out_shape=[
            jax.ShapeDtypeStruct((count, 2 * F), bf16),
            jax.ShapeDtypeStruct((40, F), f32),
            jax.ShapeDtypeStruct((count, F), bf16),
        ],
        scratch_shapes=[pltpu.VMEM((count + 8, F), f32)],
        compiler_params=grant(16),
        name="conv",
    )(normed, *arrays)


def read_kernel(heads, extra, keys, values, cums, reads, carries, gates):
    row = lax.broadcasted_iota(jnp.int32, (BLOCK, BLOCK), 0)
    col = lax.broadcasted_iota(jnp.int32, (BLOCK, BLOCK), 1)
    start = jnp.zeros((F, F), f32)
    before = jnp.zeros((1, F), f32)
    for at in range(0, heads.shape[0], BLOCK):
        part = slice(at, at + BLOCK)
        gates[part] = silu(heads[part, F:].astype(f32)) * extra[36:37]
        q = silu(heads[part, :F].astype(f32))
        k = keys[part]
        v = values[part]
        base = jnp.zeros((1, F), f32) if at % STEP == 0 else cums[at - 1 : at]
        edge = cums[at + BLOCK - 1 : at + BLOCK]
        c = cums[part] - base
        half = c[BLOCK // 2 - 1 : BLOCK // 2]
        last = edge - base
        scores = dot((q * jnp.exp(c - half)).astype(bf16), (k * jnp.exp(half - c)).astype(bf16), ((1,), (1,)))
        scores = jnp.where(row >= col, scores, 0.0).astype(bf16)
        faded = q * jnp.exp(c)
        reads[part] = dot(scores, v) + dot(faded.astype(bf16), start.astype(bf16), ((1,), (1,)))
        carries[part] = (faded * jnp.exp(before)).astype(bf16)
        fresh = dot(v, (k * jnp.exp(last - c)).astype(bf16), ((0,), (0,)))
        start = start * jnp.exp(last) + fresh
        before = before + last


def read(heads, extra, keys, values, cums):
    count = heads.shape[0]
    vmem = pl.BlockSpec(memory_space=pltpu.VMEM)
    return pl.pallas_call(
        read_kernel,
        in_specs=[vmem] * 5,
        out_specs=[vmem] * 3,
        out_shape=[
            jax.ShapeDtypeStruct((count, F), f32),
            jax.ShapeDtypeStruct((count, F), bf16),
            jax.ShapeDtypeStruct((count, F), f32),
        ],
        compiler_params=grant(12),
        name="read",
    )(heads, extra, keys, values, cums)


def row_kernel(place_ref, own, one, two, three, total, before, fade):
    _, y, _, _ = unpack_place(place_ref)
    parts = [get_message(r) for r in (own, one, two, three)]
    place = [jnp.where(y >= d, y - d, y - d + 4) for d in range(4)]
    whole, inside = 0.0, 0.0
    product, product_before = 1.0, 1.0
    for d, (state, decay) in enumerate(parts):
        later = jnp.ones_like(decay)
        between = jnp.ones_like(decay)
        for other, (_, factor) in enumerate(parts):
            if other == d:
                continue
            behind = place[other] > place[d]
            later = later * jnp.where(behind, factor, 1.0)
            between = between * jnp.where(behind & (place[other] < y), factor, 1.0)
        whole = whole + state * later
        inside = inside + state * jnp.where(place[d] < y, between, 0.0)
        product = product * decay
        product_before = product_before * jnp.where(place[d] < y, decay, 1.0)
    put_message(total, whole, product, get_rim(one))
    before[...] = inside
    fade[...] = jnp.broadcast_to(product_before, fade.shape)


def column_kernel(place_ref, own, behind, ahead, window):
    z, _, _, _ = unpack_place(place_ref)
    state, decay = get_message(behind)
    state = jnp.where(z > 0, state, 0.0)
    decay = jnp.where(z > 0, decay, 1.0)
    piece, factor = get_message(own)
    state = state * factor + piece
    decay = decay * factor
    piece, factor = get_message(ahead)
    state = jnp.where(z == ROWS - 1, piece, state * factor + piece)
    decay = jnp.where(z == ROWS - 1, factor, decay * factor)
    put_message(window, state, decay, jnp.zeros((2, F), f32))


def column(place, *messages):
    vmem = pl.BlockSpec(memory_space=pltpu.VMEM)
    return pl.pallas_call(
        column_kernel,
        in_specs=[pl.BlockSpec(memory_space=pltpu.SMEM)] + [vmem] * 3,
        out_specs=vmem,
        out_shape=jax.ShapeDtypeStruct((PACK, F), bf16),
        compiler_params=grant(4),
        name="column",
    )(place, *messages)


def join(kernel, index, *messages):
    vmem = pl.BlockSpec(memory_space=pltpu.VMEM)
    return pl.pallas_call(
        kernel,
        in_specs=[pl.BlockSpec(memory_space=pltpu.SMEM)] + [vmem] * 4,
        out_specs=[vmem] * 3,
        out_shape=[
            jax.ShapeDtypeStruct((PACK, F), bf16),
            jax.ShapeDtypeStruct((F, F), f32),
            jax.ShapeDtypeStruct((8, F), f32),
        ],
        compiler_params=grant(4),
    )(index, *messages)


def finish_kernel(place, six, three, near, row_total, row, row_fade, carries, reads, gates, extra,
                  result, window):
    z, y, _, _ = unpack_place(place)
    incoming = jnp.zeros((F, F), f32)
    for ref, least in ((six, 5), (three, 2), (near, 1)):
        piece, decay = get_message(ref)
        incoming = jnp.where(z >= least, incoming * decay + piece, incoming)
    incoming = incoming * row_fade[0:1] + row[...]
    count = reads.shape[0]
    found = reads[...] + dot(carries[...], incoming.astype(bf16), ((1,), (1,)))
    result[:count] = rms(found, gates[...]).astype(bf16)
    rim = jnp.where(y > 0, get_rim(row_total), jnp.where(z > 0, get_rim(near), 0.0))
    window[6:8] = rim
    window[8:] = extra[:16]
    total = extra[32:33] * window[6:22] + extra[33:34] * window[7:23] + extra[34:35] * window[8:24]
    result[count:] = rms(extra[16:32] * total, extra[35:36]).astype(bf16)


def finish(place, *arrays):
    vmem = pl.BlockSpec(memory_space=pltpu.VMEM)
    return pl.pallas_call(
        finish_kernel,
        in_specs=[pl.BlockSpec(memory_space=pltpu.SMEM)] + [vmem] * len(arrays),
        out_specs=vmem,
        out_shape=jax.ShapeDtypeStruct((arrays[7].shape[0] + 16, F), bf16),
        scratch_shapes=[pltpu.VMEM((24, F), f32)],
        compiler_params=grant(12),
        name="finish",
    )(place, *arrays)


def half_kernel(*refs):
    parts, weights, out = refs[:4], refs[4:8], refs[8]
    out[...] = dot(
        jnp.concatenate([r[...] for r in parts], axis=1),
        jnp.concatenate([r[F:] for r in weights], axis=0),
    )


def last_kernel(mine, *refs):
    parts, weights, earlier, out = refs[:4], refs[4:8], refs[8], refs[9]
    count, width = out.shape
    at = slice(0, width) if mine else slice(width, 2 * width)
    state = dot(
        jnp.concatenate([r[:count] for r in parts], axis=1),
        jnp.concatenate([r[:F, at] for r in weights], axis=0),
    )
    first = state[:16] + dot(
        jnp.concatenate([r[count:] for r in parts], axis=1),
        jnp.concatenate([r[F:, at] for r in weights], axis=0),
    )
    out[16:] = (earlier[16:, at] + state[16:]).astype(out.dtype)
    out[:16] = first.astype(out.dtype)


def project_half(parts, weights):
    vmem = pl.BlockSpec(memory_space=pltpu.VMEM)
    return pl.pallas_call(
        half_kernel,
        in_specs=[vmem] * 8,
        out_specs=vmem,
        out_shape=jax.ShapeDtypeStruct((parts[0].shape[0], 4 * F), f32),
        compiler_params=grant(14),
        name="half",
    )(*parts, *weights)


def project_last(mine, parts, weights, earlier):
    vmem = pl.BlockSpec(memory_space=pltpu.VMEM)
    count, width = earlier.shape
    return pl.pallas_call(
        functools.partial(last_kernel, mine),
        in_specs=[vmem] * 9,
        out_specs=vmem,
        out_shape=jax.ShapeDtypeStruct((count, width // 2), f32 if mine else bf16),
        compiler_params=grant(14),
        name="kept" if mine else "sent",
    )(*parts, *weights, earlier)


def turned(array, axis, by):
    count = lax.axis_size(axis)
    return lax.ppermute(array, axis, [(i, (i + by) % count) for i in range(count)])


def body(
    tokens,
    in_gain,
    w_query,
    w_forget,
    w_input,
    w_outgate,
    w_conv_h,
    w_conv_b,
    w_conv_c,
    forget_floor,
    forget_leak,
    state_gain,
    conv_taps,
    group_gain,
    out_state,
    out_conv,
):
    code = (lax.axis_index("z") * 4 + lax.axis_index("y")) * 4 + lax.axis_index("x")
    place = (code * 2 + lax.axis_index("c")).astype(jnp.int32).reshape(1)
    line = lambda row: row.reshape(1, -1)
    normed, scales, message, keys, values, cums, later, *columns = front(
        place,
        tokens,
        line(in_gain),
        w_forget,
        w_input,
        w_conv_h,
        w_conv_c,
        w_conv_b,
        w_query,
        w_outgate,
        line(forget_floor),
        forget_leak,
        out_state,
        out_conv,
    )
    near = [turned(message, "y", d) for d in (1, 2, 3)]
    columns = columns[:1] + [turned(columns[d], "x", d) for d in (1, 2, 3)]
    heads, extra, conv_res = conv(
        normed, scales, later, conv_taps, line(group_gain), line(state_gain)
    )
    row_total, row_before, row_fade = join(row_kernel, place, message, *near)
    near = [turned(row_total, "z", d) for d in (1, ROWS - 1)]
    conv_all = [conv_res] + [turned(conv_res, "x", d) for d in (1, 2, 3)]
    reads, carries, gates = read(heads, extra, keys, values, cums)
    window = column(place, row_total, *near)
    three, six = [turned(window, "z", d) for d in (3, 6)]
    state_res = finish(
        place, six, three, near[0], row_total, row_before, row_fade, carries, reads, gates, extra
    )
    state_all = [state_res] + [turned(state_res, "x", d) for d in (1, 2, 3)]
    half = project_half(conv_all, columns)
    sent = project_last(False, state_all, columns, half)
    got = turned(sent, "c", 1)
    kept = project_last(True, state_all, columns, half)
    return (kept + got.astype(f32)).astype(bf16)


def solution(mesh):
    assert mesh.shape["sp"] == 4 * ROWS
    chips = 4
    rows = 4
    split = Mesh(
        mesh.devices.reshape(mesh.shape["sp"] // rows, rows, chips, mesh.shape["tp"] // chips),
        ("z", "y", "x", "c"),
    )
    sp, tp = ("z", "y"), ("x", "c")
    placed = (
        P(sp, None),
        P(),
        P(None, tp),
        P(None, tp),
        P(None, tp),
        P(None, tp),
        P(None, tp),
        P(None, tp),
        P(None, tp),
        P(tp),
        P(sp, tp),
        P(),
        P(None, tp),
        P(),
        P(tp, None),
        P(tp, None),
    )
    return jax.shard_map(body, mesh=split, in_specs=placed, out_specs=P(sp, tp), check_vma=False)
```

```python
import functools

import jax
import jax.numpy as jnp
from jax import lax
from jax.experimental import pallas as pl
from jax.experimental.pallas import tpu as pltpu
from jax.sharding import Mesh
from jax.sharding import PartitionSpec as P


F = 128
BLOCK = 64
STEP = 256
FRONT = 256
PACK = F + 16
EPS = 1e-06
ROWS = 8
f32 = jnp.float32
bf16 = jnp.bfloat16


def dot(a, b, dims=((1,), (0,))):
    return lax.dot_general(a, b, (dims, ((), ())), preferred_element_type=f32)


def rms(values, gain):
    return values * lax.rsqrt(jnp.mean(values * values, axis=-1, keepdims=True) + EPS) * gain


def silu(x):
    return x * jax.nn.sigmoid(x)


def beside(ref, first, last):
    return jnp.concatenate([ref[j] for j in range(first, last)], axis=1)


def put_message(ref, state, decay, rim):
    high = decay.astype(bf16)
    low = (decay - high.astype(f32)).astype(bf16)
    ref[:F] = state.astype(bf16)
    row = lax.broadcasted_iota(jnp.int32, (16, F), 0)
    tail = jnp.where(row == 0, high.astype(f32), jnp.where(row == 1, low.astype(f32), 0.0))
    tail = jnp.where(row == 2, rim[0:1], jnp.where(row == 3, rim[1:2], tail))
    ref[F:] = tail.astype(bf16)


def get_message(ref):
    tail = ref[F:].astype(f32)
    return ref[:F].astype(f32), tail[0:1] + tail[1:2]


def get_rim(ref):
    return ref[F:].astype(f32)[2:4]


def grant(mib, **more):
    return pltpu.CompilerParams(vmem_limit_bytes=mib * 2**20, **more)


def front_kernel(place, tokens_h, gain_h, wf_h, wi_h, wh_h, wc_h, wb_h, wq_h, wg_h, floor_h, leak_h,
                 ostate_h, oconv_h,
                 tokens, scales, message, keys, values, cums, later, own, one, two, three,
                 gain, weights, floor, leak, ostate, oconv, sems):
    count, width = tokens.shape
    copies = []

    def bring(src, dst):
        copy = pltpu.make_async_copy(src, dst, sems.at[len(copies)])
        copy.start()
        copies.append(copy)
        return copy

    got_gain = bring(gain_h, gain)
    half = FRONT // 2
    got_first = [bring(tokens_h.at[pl.ds(at, half)], tokens.at[pl.ds(at, half)]) for at in (0, half)]
    got_weights = [bring(w, weights.at[j]) for j, w in enumerate((wf_h, wi_h))]
    others = [bring(floor_h, floor)]
    got_tokens = [bring(tokens_h.at[pl.ds(FRONT, FRONT)], tokens.at[pl.ds(FRONT, FRONT)])]
    others.append(bring(leak_h, leak))
    got_tokens += [
        bring(tokens_h.at[pl.ds(at, FRONT)], tokens.at[pl.ds(at, FRONT)]) for at in range(2 * FRONT, count, FRONT)
    ]
    last_copies = [bring(wh_h, later.at[0]), bring(wc_h, later.at[1])]
    last_copies += [bring(ostate_h, ostate), bring(oconv_h, oconv)]
    next_copies = [bring(w, later.at[2 + j]) for j, w in enumerate((wb_h, wq_h, wg_h))]

    row = lax.broadcasted_iota(jnp.int32, (STEP, STEP), 0)
    col = lax.broadcasted_iota(jnp.int32, (STEP, STEP), 1)
    tri = jnp.where(row >= col, 1.0, 0.0).astype(bf16)
    state = jnp.zeros((F, F), f32)
    total = jnp.zeros((1, F), f32)

    def norm(top, size):
        part = tokens[top : top + size].astype(f32)
        mean = jnp.mean(part * part, axis=-1, keepdims=True)
        scales[top : top + size] = jnp.broadcast_to(lax.rsqrt(mean + EPS), (size, F))
        tokens[top : top + size] = (part * gain[...]).astype(bf16)

    def project(top):
        scale = scales[top : top + FRONT]
        found = dot(tokens[top : top + FRONT], beside(weights, 0, 2))
        return (found * jnp.concatenate([scale, scale], axis=1)).astype(bf16)

    def gates(top, found, state, total):
        value = found[:, F:]
        values[top : top + FRONT] = value
        gate = found[:, :F].astype(f32)
        key = (1.0 - floor[...]) * jax.nn.sigmoid(-gate)
        keys[top : top + FRONT] = key
        log_forget = jnp.log1p(-key) + leak[top : top + FRONT]
        high = log_forget.astype(bf16)
        rest = log_forget - high.astype(f32)
        mid = rest.astype(bf16)
        low = (rest - mid.astype(f32)).astype(bf16)
        for at in range(0, FRONT, STEP):
            part = slice(at, at + STEP)
            cum = dot(tri, high[part]) + dot(tri, mid[part]) + dot(tri, low[part])
            cums[top + at : top + at + STEP] = cum
            last = cum[STEP - 1 : STEP]
            fresh = dot(value[part], (key[part] * jnp.exp(last - cum)).astype(bf16), ((0,), (0,)))
            state = state * jnp.exp(last) + fresh
            total = total + last
        return state, total

    got_gain.wait()
    for copy, top in zip(got_first, (0, half)):
        copy.wait()
        norm(top, half)
    for copy in got_weights:
        copy.wait()
    found = project(0)
    for top in range(FRONT, count, FRONT):
        if top == FRONT:
            for copy in others + got_tokens[:1]:
                copy.wait()
        if top == 2 * FRONT:
            for copy in got_tokens[1:]:
                copy.wait()
        norm(top, FRONT)
        following = project(top)
        state, total = gates(top - FRONT, found, state, total)
        found = following
    for copy in last_copies:
        copy.wait()
    scale = scales[count - 16 :]
    edge = dot(tokens[count - 16 :], beside(later, 0, 2)) * jnp.concatenate([scale, scale], axis=1)
    edge = edge.astype(bf16).astype(f32)
    state, total = gates(count - FRONT, found, state, total)
    put_message(message, state, jnp.exp(total), (edge[:, :F] * edge[:, F:])[14:])
    _, _, x, c = unpack_place(place)
    for d, buffer in enumerate((own, one, two, three)):
        for j in range(4):
            core = c if j < 2 else 1 - c
            at = pl.multiple_of(((x + d) & 3) * (width // 4) + core * (width // 8) + (j & 1) * F, F)
            buffer[:F, j * F : (j + 1) * F] = ostate[:, pl.ds(at, F)]
            buffer[F:, j * F : (j + 1) * F] = oconv[:, pl.ds(at, F)]
    for copy in next_copies:
        copy.wait()


def unpack_place(place):
    code = place[0]
    return code >> 5, (code >> 3) & 3, (code >> 1) & 3, code & 1


def in_hbm(arrays):
    return [pltpu.with_memory_space_constraint(a, pltpu.HBM) for a in arrays]


def front(place, *arrays):
    count, width = arrays[0].shape
    ostate = arrays[-1]
    hbm = pl.BlockSpec(memory_space=pltpu.HBM)
    vmem = pl.BlockSpec(memory_space=pltpu.VMEM)
    return pl.pallas_call(
        front_kernel,
        in_specs=[pl.BlockSpec(memory_space=pltpu.SMEM)] + [hbm] * len(arrays),
        out_specs=[vmem] * 11,
        out_shape=[
            jax.ShapeDtypeStruct((count, width), bf16),
            jax.ShapeDtypeStruct((count, F), f32),
            jax.ShapeDtypeStruct((PACK, F), bf16),
            jax.ShapeDtypeStruct((count, F), f32),
            jax.ShapeDtypeStruct((count, F), bf16),
            jax.ShapeDtypeStruct((count, F), f32),
            jax.ShapeDtypeStruct((5, width, F), bf16),
        ]
        + [jax.ShapeDtypeStruct((2 * F, 4 * F), bf16)] * 4,
        scratch_shapes=[
            pltpu.VMEM((1, width), f32),
            pltpu.VMEM((2, width, F), bf16),
            pltpu.VMEM((1, F), f32),
            pltpu.VMEM((count, F), f32),
            pltpu.VMEM(ostate.shape, bf16),
            pltpu.VMEM(ostate.shape, bf16),
            pltpu.SemaphoreType.DMA((13 + count // FRONT,)),
        ],
        compiler_params=grant(24),
        name="front",
    )(place, *in_hbm(arrays))


def conv_kernel(normed, scales, weights, taps, group, sgain, heads, extra, result, window):
    count = normed.shape[0]
    window[:8] = jnp.zeros((8, F), f32)

    def project(top, first, last):
        found = dot(normed[top : top + FRONT], beside(weights, first, last))
        return (found * jnp.concatenate([scales[top : top + FRONT]] * (last - first), axis=1)).astype(bf16)

    def convolve(top, found):
        signal = (found[:, :F].astype(f32) * found[:, F : 2 * F].astype(f32)).astype(bf16).astype(f32)
        window[8 + top : 8 + top + FRONT] = signal
        scale = taps[...].astype(f32)
        near = scale[0:1] * window[6 + top : 6 + top + FRONT]
        near = near + scale[1:2] * window[7 + top : 7 + top + FRONT]
        near = near + scale[2:3] * signal
        after = found[:, 2 * F :].astype(f32)
        result[top : top + FRONT] = rms(after * near, group[...]).astype(bf16)
        if top == 0:
            extra[:16] = signal[:16]
            extra[16:32] = after[:16]
            extra[32:35] = scale
            extra[35:36] = group[...]
            extra[36:37] = sgain[...]

    for top in range(0, count, FRONT):
        mixed = project(top, 0, 3)
        heads[top : top + FRONT] = project(top, 3, 5)
        convolve(top, mixed)


def conv(normed, *arrays):
    count, _ = normed.shape
    vmem = pl.BlockSpec(memory_space=pltpu.VMEM)
    return pl.pallas_call(
        conv_kernel,
        in_specs=[vmem] * 6,
        out_specs=[vmem] * 3,
        out_shape=[
            jax.ShapeDtypeStruct((count, 2 * F), bf16),
            jax.ShapeDtypeStruct((40, F), f32),
            jax.ShapeDtypeStruct((count, F), bf16),
        ],
        scratch_shapes=[pltpu.VMEM((count + 8, F), f32)],
        compiler_params=grant(16),
        name="conv",
    )(normed, *arrays)


def read_kernel(heads, extra, keys, values, cums, reads, carries, gates):
    row = lax.broadcasted_iota(jnp.int32, (BLOCK, BLOCK), 0)
    col = lax.broadcasted_iota(jnp.int32, (BLOCK, BLOCK), 1)
    start = jnp.zeros((F, F), f32)
    before = jnp.zeros((1, F), f32)
    for at in range(0, heads.shape[0], BLOCK):
        part = slice(at, at + BLOCK)
        gates[part] = silu(heads[part, F:].astype(f32)) * extra[36:37]
        q = silu(heads[part, :F].astype(f32))
        k = keys[part]
        v = values[part]
        base = jnp.zeros((1, F), f32) if at % STEP == 0 else cums[at - 1 : at]
        edge = cums[at + BLOCK - 1 : at + BLOCK]
        c = cums[part] - base
        half = c[BLOCK // 2 - 1 : BLOCK // 2]
        last = edge - base
        scores = dot((q * jnp.exp(c - half)).astype(bf16), (k * jnp.exp(half - c)).astype(bf16), ((1,), (1,)))
        scores = jnp.where(row >= col, scores, 0.0).astype(bf16)
        faded = q * jnp.exp(c)
        reads[part] = dot(scores, v) + dot(faded.astype(bf16), start.astype(bf16), ((1,), (1,)))
        carries[part] = (faded * jnp.exp(before)).astype(bf16)
        fresh = dot(v, (k * jnp.exp(last - c)).astype(bf16), ((0,), (0,)))
        start = start * jnp.exp(last) + fresh
        before = before + last


def read(heads, extra, keys, values, cums):
    count = heads.shape[0]
    vmem = pl.BlockSpec(memory_space=pltpu.VMEM)
    return pl.pallas_call(
        read_kernel,
        in_specs=[vmem] * 5,
        out_specs=[vmem] * 3,
        out_shape=[
            jax.ShapeDtypeStruct((count, F), f32),
            jax.ShapeDtypeStruct((count, F), bf16),
            jax.ShapeDtypeStruct((count, F), f32),
        ],
        compiler_params=grant(12),
        name="read",
    )(heads, extra, keys, values, cums)


def row_kernel(place_ref, own, one, two, three, total, before, fade):
    _, y, _, _ = unpack_place(place_ref)
    parts = [get_message(r) for r in (own, one, two, three)]
    place = [y ^ d for d in range(4)]
    whole, inside = 0.0, 0.0
    product, product_before = 1.0, 1.0
    for d, (state, decay) in enumerate(parts):
        later = jnp.ones_like(decay)
        between = jnp.ones_like(decay)
        for other, (_, factor) in enumerate(parts):
            if other == d:
                continue
            behind = place[other] > place[d]
            later = later * jnp.where(behind, factor, 1.0)
            between = between * jnp.where(behind & (place[other] < y), factor, 1.0)
        whole = whole + state * later
        inside = inside + state * jnp.where(place[d] < y, between, 0.0)
        product = product * decay
        product_before = product_before * jnp.where(place[d] < y, decay, 1.0)
    rim = jnp.where((y & 1) > 0, get_rim(one), get_rim(three))
    put_message(total, whole, product, rim)
    before[...] = inside
    fade[...] = jnp.broadcast_to(product_before, fade.shape)


def column_kernel(place_ref, own, behind, ahead, window):
    z, _, _, _ = unpack_place(place_ref)
    state, decay = get_message(behind)
    state = jnp.where(z > 0, state, 0.0)
    decay = jnp.where(z > 0, decay, 1.0)
    piece, factor = get_message(own)
    state = state * factor + piece
    decay = decay * factor
    piece, factor = get_message(ahead)
    state = jnp.where(z == ROWS - 1, piece, state * factor + piece)
    decay = jnp.where(z == ROWS - 1, factor, decay * factor)
    put_message(window, state, decay, jnp.zeros((2, F), f32))


def column(place, *messages):
    vmem = pl.BlockSpec(memory_space=pltpu.VMEM)
    return pl.pallas_call(
        column_kernel,
        in_specs=[pl.BlockSpec(memory_space=pltpu.SMEM)] + [vmem] * 3,
        out_specs=vmem,
        out_shape=jax.ShapeDtypeStruct((PACK, F), bf16),
        compiler_params=grant(4),
        name="column",
    )(place, *messages)


def join(kernel, index, *messages):
    vmem = pl.BlockSpec(memory_space=pltpu.VMEM)
    return pl.pallas_call(
        kernel,
        in_specs=[pl.BlockSpec(memory_space=pltpu.SMEM)] + [vmem] * 4,
        out_specs=[vmem] * 3,
        out_shape=[
            jax.ShapeDtypeStruct((PACK, F), bf16),
            jax.ShapeDtypeStruct((F, F), f32),
            jax.ShapeDtypeStruct((8, F), f32),
        ],
        compiler_params=grant(4),
    )(index, *messages)


def finish_kernel(place, six, three, near, row_total, row, row_fade, carries, reads, gates, extra,
                  result, window):
    z, y, _, _ = unpack_place(place)
    incoming = jnp.zeros((F, F), f32)
    for ref, least in ((six, 5), (three, 2), (near, 1)):
        piece, decay = get_message(ref)
        incoming = jnp.where(z >= least, incoming * decay + piece, incoming)
    incoming = incoming * row_fade[0:1] + row[...]
    count = reads.shape[0]
    found = reads[...] + dot(carries[...], incoming.astype(bf16), ((1,), (1,)))
    result[:count] = rms(found, gates[...]).astype(bf16)
    rim = jnp.where(y > 0, get_rim(row_total), jnp.where(z > 0, get_rim(near), 0.0))
    window[6:8] = rim
    window[8:] = extra[:16]
    total = extra[32:33] * window[6:22] + extra[33:34] * window[7:23] + extra[34:35] * window[8:24]
    result[count:] = rms(extra[16:32] * total, extra[35:36]).astype(bf16)


def finish(place, *arrays):
    vmem = pl.BlockSpec(memory_space=pltpu.VMEM)
    return pl.pallas_call(
        finish_kernel,
        in_specs=[pl.BlockSpec(memory_space=pltpu.SMEM)] + [vmem] * len(arrays),
        out_specs=vmem,
        out_shape=jax.ShapeDtypeStruct((arrays[7].shape[0] + 16, F), bf16),
        scratch_shapes=[pltpu.VMEM((24, F), f32)],
        compiler_params=grant(12),
        name="finish",
    )(place, *arrays)


def half_kernel(*refs):
    parts, weights, out = refs[:4], refs[4:8], refs[8]
    out[...] = dot(
        jnp.concatenate([r[...] for r in parts], axis=1),
        jnp.concatenate([r[F:] for r in weights], axis=0),
    )


def last_kernel(mine, *refs):
    parts, weights, earlier, out = refs[:4], refs[4:8], refs[8], refs[9]
    count, width = out.shape
    at = slice(0, width) if mine else slice(width, 2 * width)
    state = dot(
        jnp.concatenate([r[:count] for r in parts], axis=1),
        jnp.concatenate([r[:F, at] for r in weights], axis=0),
    )
    first = state[:16] + dot(
        jnp.concatenate([r[count:] for r in parts], axis=1),
        jnp.concatenate([r[F:, at] for r in weights], axis=0),
    )
    out[16:] = (earlier[16:, at] + state[16:]).astype(out.dtype)
    out[:16] = first.astype(out.dtype)


def project_half(parts, weights):
    vmem = pl.BlockSpec(memory_space=pltpu.VMEM)
    return pl.pallas_call(
        half_kernel,
        in_specs=[vmem] * 8,
        out_specs=vmem,
        out_shape=jax.ShapeDtypeStruct((parts[0].shape[0], 4 * F), f32),
        compiler_params=grant(14),
        name="half",
    )(*parts, *weights)


def project_last(mine, parts, weights, earlier):
    vmem = pl.BlockSpec(memory_space=pltpu.VMEM)
    count, width = earlier.shape
    return pl.pallas_call(
        functools.partial(last_kernel, mine),
        in_specs=[vmem] * 9,
        out_specs=vmem,
        out_shape=jax.ShapeDtypeStruct((count, width // 2), f32 if mine else bf16),
        compiler_params=grant(14),
        name="kept" if mine else "sent",
    )(*parts, *weights, earlier)


def turned(array, axis, by):
    count = lax.axis_size(axis)
    return lax.ppermute(array, axis, [(i, (i + by) % count) for i in range(count)])


def swapped(array, axis, bits):
    count = lax.axis_size(axis)
    return lax.ppermute(array, axis, [(i, i ^ bits) for i in range(count)])


def body(
    tokens,
    in_gain,
    w_query,
    w_forget,
    w_input,
    w_outgate,
    w_conv_h,
    w_conv_b,
    w_conv_c,
    forget_floor,
    forget_leak,
    state_gain,
    conv_taps,
    group_gain,
    out_state,
    out_conv,
):
    code = (lax.axis_index("z") * 4 + lax.axis_index("y")) * 4 + lax.axis_index("x")
    place = (code * 2 + lax.axis_index("c")).astype(jnp.int32).reshape(1)
    line = lambda row: row.reshape(1, -1)
    normed, scales, message, keys, values, cums, later, *columns = front(
        place,
        tokens,
        line(in_gain),
        w_forget,
        w_input,
        w_conv_h,
        w_conv_c,
        w_conv_b,
        w_query,
        w_outgate,
        line(forget_floor),
        forget_leak,
        out_state,
        out_conv,
    )
    near = [swapped(message, "y", d) for d in (1, 2, 3)]
    columns = columns[:1] + [turned(columns[d], "x", d) for d in (1, 2, 3)]
    heads, extra, conv_res = conv(
        normed, scales, later, conv_taps, line(group_gain), line(state_gain)
    )
    row_total, row_before, row_fade = join(row_kernel, place, message, *near)
    near = [turned(row_total, "z", d) for d in (1, ROWS - 1)]
    conv_all = [conv_res] + [turned(conv_res, "x", d) for d in (1, 2, 3)]
    reads, carries, gates = read(heads, extra, keys, values, cums)
    window = column(place, row_total, *near)
    three, six = [turned(window, "z", d) for d in (3, 6)]
    state_res = finish(
        place, six, three, near[0], row_total, row_before, row_fade, carries, reads, gates, extra
    )
    state_all = [state_res] + [turned(state_res, "x", d) for d in (1, 2, 3)]
    half = project_half(conv_all, columns)
    sent = project_last(False, state_all, columns, half)
    got = turned(sent, "c", 1)
    kept = project_last(True, state_all, columns, half)
    return (kept + got.astype(f32)).astype(bf16)


def solution(mesh):
    assert mesh.shape["sp"] == 4 * ROWS
    chips = 4
    rows = 4
    split = Mesh(
        mesh.devices.reshape(mesh.shape["sp"] // rows, rows, chips, mesh.shape["tp"] // chips),
        ("z", "y", "x", "c"),
    )
    sp, tp = ("z", "y"), ("x", "c")
    placed = (
        P(sp, None),
        P(),
        P(None, tp),
        P(None, tp),
        P(None, tp),
        P(None, tp),
        P(None, tp),
        P(None, tp),
        P(None, tp),
        P(tp),
        P(sp, tp),
        P(),
        P(None, tp),
        P(),
        P(tp, None),
        P(tp, None),
    )
    return jax.shard_map(body, mesh=split, in_specs=placed, out_specs=P(sp, tp), check_vma=False)
```
